128 devices in a mesh: sp: 32 (over z, y, core), tp: 4 (over x).
Axes of the slice: x: 4, y: 4, z: 4, core: 2. Of those that a mesh axis runs over, the one named last changes fastest.
Arguments:
- queries: bfloat16 [16384, 1024], P('sp', 'tp'), may hold values from -6 to 6
- keys: bfloat16 [16384, 1024], P('sp', 'tp'), may hold values from -6 to 6
- values: bfloat16 [16384, 1024], P('sp', 'tp'), may hold values from -6 to 6
- cum_gate: float32 [16384, 16], P('sp', 'tp'), as said below
- documents: int32 [16384], P('sp'), may hold values from 0 to 3, never falling along the last dimension, each value on 1 to 8192 neighbouring positions
- head_gain: float32 [1024], P('tp'), may hold values from 0.1 to 1.9
- out_weight: bfloat16 [1024, 2048], replicated, may hold values from -0.1875 to 0.1875
- resid: bfloat16 [16384, 2048], P(('sp', 'tp')), may hold values from -6 to 6
- norm_gain: float32 [2048], replicated, may hold values from 0.1 to 1.9
- routes: int32 [16384, 2], P(('sp', 'tp')), may hold values from 0 to 31, all different within a row; in each aligned block of 128 rows (0 to 127, 128 to 255, ...) at most 16 rows name the same one
- route_weights: float32 [16384, 2], P(('sp', 'tp')), may hold values from 0.25 to 1
- w_gate: bfloat16 [32, 2048, 3584], P('sp', None, 'tp'), may hold values from -0.125 to 0.125
- w_up: bfloat16 [32, 2048, 3584], P('sp', None, 'tp'), may hold values from -0.125 to 0.125
- w_down: bfloat16 [32, 3584, 2048], P('sp', 'tp'), may hold values from -0.09375 to 0.09375
Outputs:
- mixed: bfloat16 [16384, 2048], P(('sp', 'tp'))
The draws below stay inside these ranges and needn't reach their ends.
Inputs may be any that keep to these rules, and one draw needn't show every extreme that they name: `cum_gate`: along the positions each head's values never rise. `documents`: document numbers never fall along the positions. `routes`: the 2 experts of a row differ. In each aligned block of 128 rows no expert is named more than 16 times; in some blocks an expert is named exactly 16 times.
All inputs are finite; a program needn't handle non-finite values.
Results may differ from the reference program's by a relative error of at most 0.015.
Values may be sent and summed in bfloat16 or wider, within the bound.
A program may use at most 128 MiB of HBM per device.

```python
import math
import jax
import jax.numpy as jnp
import numpy as np
from jax import lax

D = 2048
HEADS = 16
HEAD_DIM = 64
FFE = 3584
TOP = 2
TOK_DEV = 512
SEQUENCE_LENGTH = 16384
ROWS_DEV = 128
HD = 1024
EXPERTS = 32
CAP = 16
SLICE = 896
N_SP = 32
N_TP = 4


def draw_queries(key, part):
    drawn = jax.random.normal(jax.random.fold_in(key, 1), (SEQUENCE_LENGTH, HEADS * HEAD_DIM), jnp.float32)
    return jnp.clip(drawn, -6.0, 6.0).astype(jnp.bfloat16)


def draw_keys(key, part):
    drawn = jax.random.normal(jax.random.fold_in(key, 2), (SEQUENCE_LENGTH, HEADS * HEAD_DIM), jnp.float32)
    return jnp.clip(drawn, -6.0, 6.0).astype(jnp.bfloat16)


def draw_cum_gate(key, part):
    head_order = jax.random.permutation(jax.random.fold_in(key, 21), HEADS)
    fast_heads = head_order < HEADS // 2
    quick_decay_rate = jnp.exp(jax.random.uniform(jax.random.fold_in(key, 22), (HEADS,), jnp.float32, math.log(0.03), math.log(0.08)))
    slow_rate = jax.random.uniform(jax.random.fold_in(key, 23), (HEADS,), jnp.float32, 0.3, 0.8) / SEQUENCE_LENGTH
    head_rates = jnp.where(fast_heads, quick_decay_rate, slow_rate)
    blocks = SEQUENCE_LENGTH // TOK_DEV
    factor = jnp.exp(jax.random.uniform(jax.random.fold_in(key, 24), (blocks, HEADS), jnp.float32, -0.7, 0.7))
    factor = jnp.repeat(factor, TOK_DEV, axis=0)
    jitter = jax.random.uniform(jax.random.fold_in(key, 25), (SEQUENCE_LENGTH, HEADS), jnp.float32, 0.5, 1.5)
    logged_step_list = -head_rates[None, :] * factor * jitter
    spike_position = jax.random.randint(jax.random.fold_in(key, 26), (3,), 0, SEQUENCE_LENGTH)
    loss_values = jax.random.uniform(jax.random.fold_in(key, 27), (3, HEADS), jnp.float32, 0.2, 0.5)
    logged_step_list = logged_step_list.at[spike_position].add(jnp.log(1.0 - loss_values))
    return jnp.cumsum(logged_step_list, axis=0)


def block_scale(stream_key, shape, shards, smallest, high):
    factor_of = 1.0
    for axis_at, shards_of in shards:
        heights = jax.random.uniform(jax.random.fold_in(jax.random.fold_in(stream_key, 6), axis_at), (shards_of,), jnp.float32, smallest / len(shards), high / len(shards))
        factor_of = factor_of * jnp.repeat(jnp.exp(heights), shape[axis_at] // shards_of).reshape((-1,) + (1,) * (len(shape) - 1 - axis_at))
    return factor_of


def length_profile(count, total, reach, slope):
    loads = [(1 << 20) // math.isqrt(rank ** slope) + 1 for rank in range(2, count + 1)]
    spare, given = total - reach - (count - 1), [1] * (count - 1)
    while spare > 0:
        candidates = [i for i in range(count - 1) if given[i] < reach]
        pool, left = sum([loads[i] for i in candidates]), spare
        for i in candidates:
            addition = min(reach - given[i], max(1, left * loads[i] // pool), spare)
            given[i] = given[i] + addition
            spare = spare - addition
    return np.array([reach] + given)


def ragged_sizes(own_key, count, total, bound, lean):
    if count == 2:
        one = jax.random.randint(own_key, (), max(1, total - bound), min(bound, total - 1) + 1)
        return jnp.stack([one, total - one])
    sizes = jnp.asarray(length_profile(count, total, bound, lean), jnp.int32)
    twos = (count - 1) // 2
    source_of, taker = sizes[1:1 + 2 * twos:2], sizes[2:2 + 2 * twos:2]
    margin = jnp.minimum(source_of - 1, bound - taker)
    shifted = jax.random.randint(jax.random.fold_in(own_key, 1), (twos,), 0, 1 << 20) % (margin + 1)
    sizes = sizes.at[1:1 + 2 * twos:2].set(source_of - shifted).at[2:2 + 2 * twos:2].set(taker + shifted)
    return sizes[jax.random.permutation(jax.random.fold_in(own_key, 2), count)]


def shared_out(own_key, own, number, rows, count, top, most, lean):
    sequence = jax.random.permutation(own_key, count)
    heavy_load, usual = shares(count, rows * top, most, lean, True), shares(count, rows * top, most, lean, False)
    places = jnp.arange(count)

    def named(tallies, offset_by):
        used = int((tallies > 0).sum())
        fixed = max(1, used // 4)
        passed = fixed + (places - fixed + offset_by * (used - fixed)) % max(1, count - fixed)
        return jnp.zeros((count,), jnp.int32).at[sequence[jnp.where(places < fixed, places, passed)]].set(jnp.asarray(tallies, jnp.int32))

    tallies = jnp.where(number % 4 == 0, named(heavy_load, number // 4), named(usual, number - number // 4 - 1))
    mixed = jax.random.permutation(jax.random.fold_in(own, 3), count)
    source_of, sink = mixed[0:count // 2 * 2:2], mixed[1:count // 2 * 2:2]
    room = jnp.minimum(tallies[source_of] - 1, most - tallies[sink]) // 2
    room = jnp.where((source_of == sequence[0]) | (sink == sequence[0]) | (tallies[sink] == 0), 0, jnp.maximum(room, 0))
    passed = jax.random.randint(jax.random.fold_in(own, 4), (count // 2,), 0, 1 << 20) % (room + 1)
    tallies = tallies.at[source_of].add(-passed).at[sink].add(passed)
    labels = jnp.searchsorted(jnp.cumsum(tallies), jnp.arange(rows * top), side="right").astype(jnp.int32)
    table = labels.reshape(top, rows).T
    table = table[jax.random.permutation(jax.random.fold_in(own, 1), rows)]
    offset_by = jax.random.randint(jax.random.fold_in(own, 2), (rows, 1), 0, top)
    return jnp.take_along_axis(table, (jnp.arange(top)[None, :] + offset_by) % top, axis=1)


def shares(amount, total, limit, slope, full):
    portions = [(1 << 20) // math.isqrt(grade ** slope) + 1 for grade in range(1, amount + 1)]
    largest = limit if full else min(limit, max(-(-total // amount), total * portions[0] // sum(portions)))
    least = 1 if total - largest >= amount - 1 else 0
    counts, spare = [largest] + [least] * (amount - 1), total - largest - least * (amount - 1)
    while spare > 0:
        free = [i for i in range(1, amount) if counts[i] < largest] or [i for i in range(1, amount) if counts[i] < limit]
        whole, remaining = sum([portions[i] for i in free]), spare
        for i in free:
            extra = min(limit - counts[i], max(1, remaining * portions[i] // whole), spare)
            counts[i] = counts[i] + extra
            spare = spare - extra
    return np.array(counts)


def noise(stream_key, dims, spread, bound, split=(), held_as=jnp.bfloat16):
    entries = jax.random.normal(stream_key, dims, jnp.float32) * spread
    if len(split) > 0:
        entries = block_scale(stream_key, dims, split, -0.22, 0.18) * entries
    return jnp.clip(entries, min=-bound, max=bound).astype(held_as)


def setup_inputs(seed: int = 0) -> dict:
    seeds = jax.random.split(jax.random.key(seed), 15)
    queries = draw_queries(jax.random.fold_in(seeds[14], 71), 0)
    keys = draw_keys(jax.random.fold_in(seeds[14], 71), 0)
    values = noise(seeds[2], (SEQUENCE_LENGTH, HD), 1.0, 6.0, ((0, 32), (1, 4)))
    cum_gate = draw_cum_gate(jax.random.fold_in(seeds[14], 71), 0)
    documents = jnp.searchsorted(jnp.cumsum(ragged_sizes(seeds[4], 4, SEQUENCE_LENGTH, SEQUENCE_LENGTH // 2, 2)), jnp.arange(SEQUENCE_LENGTH), side="right").astype(jnp.int32)
    head_gain = jnp.clip(1.0 + 0.18 * jax.random.normal(seeds[5], (HD,), jnp.float32), 0.1, 1.9)
    out_weight = noise(seeds[6], (HD, D), HD ** -0.5, 0.1875)
    resid = noise(seeds[7], (SEQUENCE_LENGTH, D), 1.0, 6.0, ((0, 128),))
    norm_gain = jnp.clip(1.0 + 0.18 * jax.random.normal(seeds[8], (D,), jnp.float32), 0.1, 1.9)
    routes_keys = jax.random.split(jax.random.fold_in(seeds[9], 1), SEQUENCE_LENGTH // ROWS_DEV)
    routes_turns = jax.random.permutation(jax.random.fold_in(seeds[9], 3), SEQUENCE_LENGTH // ROWS_DEV)
    routes = jax.vmap(lambda own, number: shared_out(jax.random.fold_in(seeds[9], 2), own, number, ROWS_DEV, EXPERTS, TOP, CAP, 2))(routes_keys, routes_turns).reshape((SEQUENCE_LENGTH, TOP))
    route_weights = jnp.clip(jnp.exp(math.log(1.0) - 1.3862944 * jax.random.uniform(seeds[10], (SEQUENCE_LENGTH, TOP), jnp.float32) ** block_scale(seeds[10], (SEQUENCE_LENGTH, TOP), ((0, 128),), -0.2, 0.2)), 0.25, 1.0)
    w_gate = noise(seeds[11], (EXPERTS, D, FFE), D ** -0.5, 0.125, ((0, 32), (2, 4)))
    w_up = noise(seeds[12], (EXPERTS, D, FFE), D ** -0.5, 0.125, ((0, 32), (2, 4)))
    w_down = noise(seeds[13], (EXPERTS, FFE, D), FFE ** -0.5, 0.09375, ((0, 32), (1, 4)))
    return dict(queries=queries, keys=keys, values=values, cum_gate=cum_gate, documents=documents, head_gain=head_gain, out_weight=out_weight, resid=resid, norm_gain=norm_gain, routes=routes, route_weights=route_weights, w_gate=w_gate, w_up=w_up, w_down=w_down)


EPS = 1e-06

def attention(queries, keys, values, cum_gate, documents):
    block_len = math.gcd(SEQUENCE_LENGTH, 256)
    block_count = SEQUENCE_LENGTH // block_len
    key_heads = keys.reshape(SEQUENCE_LENGTH, HEADS, HEAD_DIM).astype(jnp.float32)
    value_heads = values.reshape(SEQUENCE_LENGTH, HEADS, HEAD_DIM).astype(jnp.float32)
    positions = jnp.arange(SEQUENCE_LENGTH, dtype=jnp.int32)
    score_scale = HEAD_DIM ** (-0.5)

    def one_block(block_index):
        first_pos = block_index * block_len
        query_row_block = lax.dynamic_slice_in_dim(queries, first_pos, block_len, 0)
        query_row_block = query_row_block.reshape(block_len, HEADS, HEAD_DIM).astype(jnp.float32)
        gate_here = lax.dynamic_slice_in_dim(cum_gate, first_pos, block_len, 0)
        doc_here = lax.dynamic_slice_in_dim(documents, first_pos, block_len, 0)
        query_pos = first_pos + jnp.arange(block_len, dtype=jnp.int32)
        scores = jnp.einsum('qhd,khd->qhk', query_row_block, key_heads) * score_scale
        scores = scores + gate_here[:, :, None] - cum_gate.T[None, :, :]
        allowed = (positions[None, :] <= query_pos[:, None]) & (documents[None, :] == doc_here[:, None])
        scores = jnp.where(allowed[:, None, :], scores, -jnp.inf)
        row_max = lax.optimization_barrier(jnp.max(scores, axis=-1, keepdims=True))
        exp_scores = jnp.exp(scores - row_max)
        row_sum = lax.optimization_barrier(jnp.sum(exp_scores, axis=-1))
        weights = lax.optimization_barrier(exp_scores.astype(jnp.bfloat16)).astype(jnp.float32)
        return jnp.einsum('qhk,khd->qhd', weights, value_heads) / row_sum[:, :, None]
    attended = lax.map(one_block, jnp.arange(block_count, dtype=jnp.int32))
    return attended.reshape(SEQUENCE_LENGTH, HEADS, HEAD_DIM)

def experts_out(expert_input, routes, w_gate, w_up, w_down):
    capacity = N_SP * N_TP * CAP
    flat_routes = routes.reshape(-1)
    route_total = flat_routes.shape[0]
    owners = jnp.arange(route_total, dtype=jnp.int32) // TOP

    def one_expert(expert_index):
        matches = (flat_routes == expert_index).astype(jnp.int32)
        ranks = jnp.cumsum(matches) - 1
        slots = jnp.where(matches == 1, ranks, capacity)
        slot_owner = jnp.zeros((capacity + 1,), jnp.int32).at[slots].set(owners)[:capacity]
        picked = expert_input[slot_owner]
        gate_out = jnp.dot(picked, w_gate[expert_index], preferred_element_type=jnp.float32)
        up_out = jnp.dot(picked, w_up[expert_index], preferred_element_type=jnp.float32)
        hidden = (jax.nn.silu(gate_out) * up_out).astype(jnp.bfloat16)
        pieces = hidden.reshape(capacity, N_TP, SLICE).astype(jnp.float32)
        down_blocks = w_down[expert_index].reshape(N_TP, SLICE, D).astype(jnp.float32)
        partial_value = jnp.einsum('rjf,jfd->jrd', pieces, down_blocks)
        partial_value = lax.optimization_barrier(partial_value.astype(jnp.bfloat16)).astype(jnp.float32)
        return lax.optimization_barrier(jnp.sum(partial_value, axis=0)).astype(jnp.bfloat16)
    results = lax.map(one_expert, jnp.arange(EXPERTS, dtype=jnp.int32))
    onehot = (flat_routes[:, None] == jnp.arange(EXPERTS, dtype=jnp.int32)[None, :]).astype(jnp.int32)
    ranks = lax.optimization_barrier(jnp.sum(jnp.cumsum(onehot, axis=0) * onehot, axis=1)) - 1
    return results[flat_routes, ranks].reshape(SEQUENCE_LENGTH, TOP, D)

def reference(queries, keys, values, cum_gate, documents, head_gain, out_weight, resid, norm_gain, routes, route_weights, w_gate, w_up, w_down):
    attended = attention(queries, keys, values, cum_gate, documents)
    mean_square = lax.optimization_barrier(jnp.mean(attended * attended, axis=-1, keepdims=True))
    head_normed = (attended * lax.rsqrt(mean_square + EPS)).reshape(SEQUENCE_LENGTH, HEADS * HEAD_DIM) * head_gain
    head_normed = head_normed.astype(jnp.bfloat16)
    projected = jnp.dot(head_normed, out_weight, preferred_element_type=jnp.float32)
    stream = lax.optimization_barrier((resid.astype(jnp.float32) + projected).astype(jnp.bfloat16))
    widened = stream.astype(jnp.float32)
    mean_wide = lax.optimization_barrier(jnp.mean(widened * widened, axis=-1, keepdims=True))
    expert_input = (widened * lax.rsqrt(mean_wide + EPS) * norm_gain).astype(jnp.bfloat16)
    gathered = experts_out(expert_input, routes, w_gate, w_up, w_down)
    mixed = widened + lax.optimization_barrier(jnp.sum(route_weights[:, :, None] * gathered.astype(jnp.float32), axis=1))
    return mixed.astype(jnp.bfloat16)
```

```python
import jax
import jax.numpy as jnp
from jax import lax
from jax.experimental import pallas as pl
from jax.experimental.pallas import tpu as pltpu
from jax.sharding import PartitionSpec as P

EPS = 1e-06
LOG2E = 1.4426950408889634
BLK = 512
EXTRA = 32
NEG = -1e30
F32 = jnp.float32
BF16 = jnp.bfloat16


def pieces_of(x):
    hi = lax.reduce_precision(x, 8, 7)
    rest = x - hi
    mid = lax.reduce_precision(rest, 8, 7)
    return hi, mid, rest - mid


def attention_kernel(q_ref, kvx_ref, gain_ref, o_ref, kp, vt, qp, acc, mrow, g0):
    members = kvx_ref.shape[0]
    groups = kvx_ref.shape[1]
    blocks = members * groups
    me = lax.rem(lax.axis_index("sp"), members)
    lane = lax.broadcasted_iota(jnp.int32, (128, 128), 1)
    lane_wide = lax.broadcasted_iota(jnp.int32, (BLK, 128), 1)
    row_extra = lax.broadcasted_iota(jnp.int32, (EXTRA, 128), 0)
    is_doc = (row_extra >= 12) & (row_extra < 16)

    def prepare(kb, counts):
        member, group = lax.rem(kb, members), kb // members
        extra = kvx_ref[member, group, BLK : BLK + EXTRA, :].astype(F32)
        g0[kb] = jnp.sum(jnp.where(row_extra == 16, extra, 0.0))
        counts = tuple(
            count + jnp.where(is_doc & (extra < d + 0.5), 1.0, 0.0)
            for d, count in enumerate(counts)
        )
        turned = jnp.concatenate([extra, jnp.zeros((128 - EXTRA, 128), F32)], axis=0).T
        for c in range(4):
            kp[kb, c * 128 : (c + 1) * 128, 128:256] = jnp.where(
                (lane < 12) & (lane % 4 == c), turned, 0.0
            ).astype(BF16)
        kv = kvx_ref[member, group, 0:BLK, :].astype(F32)
        kp[kb, :, 0:128] = jnp.where(lane_wide < 64, kv, pltpu.roll(kv, 64, 1)).astype(BF16)
        vt[kb, 16:80, :] = kv.T[64:128, :].astype(BF16)
        vt[kb, 0:16, :] = jnp.ones((16, BLK), BF16)
        return counts

    zero = jnp.zeros((EXTRA, 128), F32)
    counts = lax.fori_loop(0, blocks, prepare, (zero, zero, zero))
    starts = [jnp.sum(c).astype(jnp.int32) for c in counts]

    def one_query_block(i, unused):
        qb = i * members + me
        half = q_ref[i].astype(F32) * (LOG2E * 0.125)
        q = jnp.concatenate([half, pltpu.roll(half, 64, 1)], axis=0)
        hi = q.astype(BF16).astype(F32)
        low = pltpu.roll(q - hi, 64, 1)
        qp[:, 0:128] = jnp.where(lane_wide < 64, hi, low).astype(BF16)
        qp[:, 128:256] = jnp.where(lane_wide < 12, 1.0, 0.0).astype(BF16)
        extra = kvx_ref[me, i, BLK : BLK + EXTRA, :].astype(F32)
        doc = jnp.concatenate([extra[12 + c : 13 + c, :] for c in range(4)], axis=1)
        start = jnp.where(
            doc < 0.5,
            0,
            jnp.where(doc < 1.5, starts[0], jnp.where(doc < 2.5, starts[1], starts[2])),
        )
        first = jnp.min(start)
        last = jnp.max(start)
        base = g0[qb]

        def visit(kb, masked, fresh):
            shift = (base - g0[kb]) * LOG2E
            scores = lax.dot_general(
                kp[kb], qp[...], (((1,), (1,)), ((), ())), preferred_element_type=F32
            )
            if masked:
                key_pos = kb * BLK + lax.broadcasted_iota(jnp.int32, (BLK, BLK), 0)
                query_pos = qb * BLK + lax.broadcasted_iota(jnp.int32, (BLK, BLK), 1)
                allowed = (key_pos <= query_pos) & (key_pos >= start)
                scores = jnp.where(allowed, scores, NEG)
            top = jnp.max(scores, axis=0, keepdims=True) + shift
            if not fresh:
                old = mrow[...]
                top = jnp.maximum(old, top)
            weights = jnp.exp2(scores - (top - shift)).astype(BF16)
            added = jnp.dot(vt[kb], weights, preferred_element_type=F32)
            if fresh:
                acc[...] = added
            else:
                acc[...] = acc[...] * jnp.exp2(old - top) + added
            mrow[...] = top

        visit(qb, True, True)

        def earlier(kb, carry):
            plain = kb * BLK >= last

            @pl.when(plain)
            def _():
                visit(kb, False, False)

            @pl.when(jnp.logical_not(plain))
            def _():
                visit(kb, True, False)

            return carry

        lax.fori_loop(first // BLK, qb, earlier, 0)
        out = acc[16:80, :] / acc[0:1, :]
        mean_square = jnp.mean(out * out, axis=0, keepdims=True)
        gain = jnp.concatenate([gain_ref[...]] * 4, axis=1)
        o_ref[i] = (out * lax.rsqrt(mean_square + EPS) * gain).astype(BF16)
        return unused

    lax.fori_loop(0, groups, one_query_block, 0)


def attend(q, kvx, gain):
    members, groups = kvx.shape[:2]
    blocks = members * groups
    vmem = pl.BlockSpec(memory_space=pltpu.VMEM)
    return pl.pallas_call(
        attention_kernel,
        out_shape=jax.ShapeDtypeStruct((groups, 64, BLK), BF16),
        in_specs=[vmem] * 3,
        out_specs=vmem,
        scratch_shapes=[
            pltpu.VMEM((blocks, BLK, 256), BF16),
            pltpu.VMEM((blocks, 80, BLK), BF16),
            pltpu.VMEM((BLK, 256), BF16),
            pltpu.VMEM((80, BLK), F32),
            pltpu.VMEM((1, BLK), F32),
            pltpu.SMEM((blocks,), F32),
        ],
        compiler_params=pltpu.CompilerParams(vmem_limit_bytes=48 * 1024 * 1024),
        name="attention",
    )(q, kvx, gain)


def items_in_groups(shard, axis, split_dim, concat_dim, work, item_dim, out_dim):

    def moved(group):
        return lax.all_to_all(group, axis, split_axis=split_dim, concat_axis=concat_dim, tiled=True)

    items = jax.tree.leaves(shard)[0].shape[item_dim]
    ends = [items * k // 4 for k in range(4 + 1)] if items % 4 == 0 else [0, items]
    groups = [
        jax.tree.map(lambda a: lax.slice_in_dim(a, low, high, axis=item_dim), shard)
        for low, high in zip(ends, ends[1:])
    ]
    arrived = [moved(group) for group in groups]
    made = [work(group) for group in arrived]
    return jax.tree.map(lambda *parts: jnp.concatenate(parts, axis=out_dim), *made)


def on_device(
    queries,
    keys,
    values,
    cum_gate,
    documents,
    head_gain,
    out_weight,
    resid,
    norm_gain,
    routes,
    route_weights,
    w_gate,
    w_up,
    w_down,
):
    tokens = queries.shape[0]
    heads = cum_gate.shape[1]
    sp_count = lax.axis_size("sp")
    members = sp_count // heads
    z = lax.axis_index("sp") // members

    def by_head(a):
        return a.reshape(tokens, heads, 64).transpose(1, 0, 2)

    qh = by_head(queries)
    q_pack = jnp.concatenate([qh[:, : BLK // 2], qh[:, BLK // 2 :]], axis=-1)
    kv = jnp.concatenate([by_head(keys), by_head(values)], axis=-1)
    gate = cum_gate.T
    gate0 = gate[:, :1]
    rel = jnp.stack(pieces_of((gate0 - gate) * LOG2E), axis=1).reshape(heads, 12, 128)
    docs = jnp.broadcast_to(documents.astype(F32).reshape(1, 4, 128), (heads, 4, 128))
    zero_row = jnp.pad(jnp.stack(pieces_of(gate0), axis=2), ((0, 0), (0, 15), (0, 125)))
    extra = jnp.concatenate([rel, docs, zero_row], axis=1).astype(BF16)
    payload = jnp.concatenate([kv, extra, q_pack], axis=1)
    columns = [[j + members * g for g in range(heads)] for j in range(members)]
    rows = [[j + members * g for j in range(members)] for g in range(heads)]
    arrived = lax.all_to_all(
        payload, "sp", split_axis=0, concat_axis=0, axis_index_groups=columns, tiled=True
    )
    kvx = lax.all_gather(arrived[:, : BLK + EXTRA], "sp", axis=0, axis_index_groups=rows)
    gain = jnp.broadcast_to(lax.dynamic_slice_in_dim(head_gain, z * 64, 64)[:, None], (64, 128))
    normed = attend(arrived[:, BLK + EXTRA :], kvx, gain)
    normed = lax.all_to_all(
        normed, "sp", split_axis=0, concat_axis=0, axis_index_groups=columns, tiled=True
    ).reshape(heads * 64, tokens)
    tp_count = lax.axis_size("tp")
    local_rows = tokens // tp_count
    regrouped = lax.all_to_all(normed, "tp", split_axis=1, concat_axis=0, tiled=True)
    projected = lax.dot_general(
        regrouped, out_weight, (((0,), (0,)), ((), ())), preferred_element_type=F32
    )
    stream = lax.optimization_barrier((resid.astype(F32) + projected).astype(BF16))
    widened = stream.astype(F32)
    mean_wide = jnp.mean(widened * widened, axis=-1, keepdims=True)
    expert_input = (widened * lax.rsqrt(mean_wide + EPS) * norm_gain).astype(BF16)
    top_count = routes.shape[1]
    expert_count = sp_count
    model_width = stream.shape[1]
    capacity = 2 * top_count * tokens // (tp_count * expert_count)
    flat_routes = routes.reshape(-1)
    route_total = flat_routes.shape[0]
    onehot = (flat_routes[:, None] == jnp.arange(expert_count, dtype=jnp.int32)[None, :]).astype(
        jnp.int32
    )
    ranks = jnp.sum(jnp.cumsum(onehot, axis=0) * onehot, axis=1) - 1
    targets = flat_routes * capacity + ranks
    owners = jnp.arange(route_total, dtype=jnp.int32) // top_count
    slot_owner = jnp.zeros((expert_count * capacity,), jnp.int32).at[targets].set(owners)
    slot_used = jnp.zeros((expert_count * capacity,), jnp.bool_).at[targets].set(True)
    outbound = jnp.where(slot_used[:, None], expert_input[slot_owner], jnp.zeros((), BF16))
    outbound = outbound.reshape(expert_count, capacity, model_width)

    def expert_rows(arrived):
        flat_rows = arrived.reshape(-1, model_width)
        gate_out = jnp.dot(flat_rows, w_gate[0], preferred_element_type=F32)
        up_out = jnp.dot(flat_rows, w_up[0], preferred_element_type=F32)
        hidden = (jax.nn.silu(gate_out) * up_out).astype(BF16)
        partial_value = jnp.dot(hidden, w_down[0], preferred_element_type=F32)
        partial_value = lax.optimization_barrier(partial_value.astype(BF16)).astype(F32)
        return partial_value.reshape(arrived.shape)

    def finish(partial_value):
        summed = lax.psum_scatter(
            partial_value.astype(BF16), "tp", scatter_dimension=1, tiled=True
        ).astype(F32)
        return lax.all_to_all(
            summed[:, 0].astype(BF16), "sp", split_axis=0, concat_axis=0, tiled=True
        )

    def at_experts(arrived):
        fanned = lax.all_gather(arrived[:, None], "tp", axis=1, tiled=True)
        return finish(expert_rows(fanned))

    returned = items_in_groups(outbound, "sp", 0, 0, at_experts, 1, 1)
    results = returned.reshape(expert_count * capacity, model_width)[targets]
    results = results.reshape(local_rows, top_count, model_width)
    mixed = widened + jnp.sum(route_weights[:, :, None] * results.astype(F32), axis=1)
    return mixed.astype(BF16)


def solution(mesh):
    in_specs = (
        P("sp", "tp"),
        P("sp", "tp"),
        P("sp", "tp"),
        P("sp", "tp"),
        P("sp"),
        P("tp"),
        P(),
        P(("sp", "tp"), None),
        P(),
        P(("sp", "tp"), None),
        P(("sp", "tp"), None),
        P("sp", None, "tp"),
        P("sp", None, "tp"),
        P("sp", "tp", None),
    )
    out_specs = P(("sp", "tp"), None)
    return jax.shard_map(
        on_device, mesh=mesh, in_specs=in_specs, out_specs=out_specs, check_vma=False
    )
```

```python
import jax
import jax.numpy as jnp
from jax import lax
from jax.experimental import pallas as pl
from jax.experimental.pallas import tpu as pltpu
from jax.sharding import PartitionSpec as P

EPS = 1e-06
LOG2E = 1.4426950408889634
BLK = 512
EXTRA = 32
NEG = -1e30
F32 = jnp.float32
BF16 = jnp.bfloat16


def pieces_of(x):
    hi = lax.reduce_precision(x, 8, 7)
    rest = x - hi
    mid = lax.reduce_precision(rest, 8, 7)
    return hi, mid, rest - mid


def attention_kernel(q_ref, kvx_ref, gain_ref, o_ref, kp, vt, qp, acc, mrow, g0):
    members = kvx_ref.shape[0]
    groups = kvx_ref.shape[1]
    blocks = members * groups
    me = lax.rem(lax.axis_index("sp"), members)
    lane = lax.broadcasted_iota(jnp.int32, (128, 128), 1)
    lane_wide = lax.broadcasted_iota(jnp.int32, (BLK, 128), 1)
    row_extra = lax.broadcasted_iota(jnp.int32, (EXTRA, 128), 0)
    is_doc = (row_extra >= 12) & (row_extra < 16)

    def prepare(kb, counts):
        member, group = lax.rem(kb, members), kb // members
        extra = kvx_ref[member, group, BLK : BLK + EXTRA, :].astype(F32)
        g0[kb] = jnp.sum(jnp.where(row_extra == 16, extra, 0.0))
        counts = tuple(
            count + jnp.where(is_doc & (extra < d + 0.5), 1.0, 0.0)
            for d, count in enumerate(counts)
        )
        turned = jnp.concatenate([extra, jnp.zeros((128 - EXTRA, 128), F32)], axis=0).T
        for c in range(4):
            kp[kb, c * 128 : (c + 1) * 128, 128:256] = jnp.where(
                (lane < 12) & (lane % 4 == c), turned, 0.0
            ).astype(BF16)
        kv = kvx_ref[member, group, 0:BLK, :].astype(F32)
        kp[kb, :, 0:128] = jnp.where(lane_wide < 64, kv, pltpu.roll(kv, 64, 1)).astype(BF16)
        vt[kb, 16:80, :] = kv.T[64:128, :].astype(BF16)
        vt[kb, 0:16, :] = jnp.ones((16, BLK), BF16)
        return counts

    zero = jnp.zeros((EXTRA, 128), F32)
    counts = lax.fori_loop(0, blocks, prepare, (zero, zero, zero))
    starts = [jnp.sum(c).astype(jnp.int32) for c in counts]

    def one_query_block(i, unused):
        qb = i * members + me
        half = q_ref[i].astype(F32) * (LOG2E * 0.125)
        q = jnp.concatenate([half, pltpu.roll(half, 64, 1)], axis=0)
        hi = q.astype(BF16).astype(F32)
        low = pltpu.roll(q - hi, 64, 1)
        qp[:, 0:128] = jnp.where(lane_wide < 64, hi, low).astype(BF16)
        qp[:, 128:256] = jnp.where(lane_wide < 12, 1.0, 0.0).astype(BF16)
        extra = kvx_ref[me, i, BLK : BLK + EXTRA, :].astype(F32)
        doc = jnp.concatenate([extra[12 + c : 13 + c, :] for c in range(4)], axis=1)
        start = jnp.where(
            doc < 0.5,
            0,
            jnp.where(doc < 1.5, starts[0], jnp.where(doc < 2.5, starts[1], starts[2])),
        )
        first = jnp.min(start)
        last = jnp.max(start)
        base = g0[qb]

        def visit(kb, masked, fresh):
            shift = (base - g0[kb]) * LOG2E
            scores = lax.dot_general(
                kp[kb], qp[...], (((1,), (1,)), ((), ())), preferred_element_type=F32
            )
            if masked:
                key_pos = kb * BLK + lax.broadcasted_iota(jnp.int32, (BLK, BLK), 0)
                query_pos = qb * BLK + lax.broadcasted_iota(jnp.int32, (BLK, BLK), 1)
                allowed = (key_pos <= query_pos) & (key_pos >= start)
                scores = jnp.where(allowed, scores, NEG)
            top = jnp.max(scores, axis=0, keepdims=True) + shift
            if not fresh:
                old = mrow[...]
                top = jnp.maximum(old, top)
            weights = jnp.exp2(scores - (top - shift)).astype(BF16)
            added = jnp.dot(vt[kb], weights, preferred_element_type=F32)
            if fresh:
                acc[...] = added
            else:
                acc[...] = acc[...] * jnp.exp2(old - top) + added
            mrow[...] = top

        visit(qb, True, True)

        def earlier(kb, carry):
            plain = kb * BLK >= last

            @pl.when(plain)
            def _():
                visit(kb, False, False)

            @pl.when(jnp.logical_not(plain))
            def _():
                visit(kb, True, False)

            return carry

        lax.fori_loop(first // BLK, qb, earlier, 0)
        out = acc[16:80, :] / acc[0:1, :]
        mean_square = jnp.mean(out * out, axis=0, keepdims=True)
        gain = jnp.concatenate([gain_ref[...]] * 4, axis=1)
        o_ref[i] = (out * lax.rsqrt(mean_square + EPS) * gain).astype(BF16)
        return unused

    lax.fori_loop(0, groups, one_query_block, 0)


def attend(q, kvx, gain):
    members, groups = kvx.shape[:2]
    blocks = members * groups
    vmem = pl.BlockSpec(memory_space=pltpu.VMEM)
    return pl.pallas_call(
        attention_kernel,
        out_shape=jax.ShapeDtypeStruct((groups, 64, BLK), BF16),
        in_specs=[vmem] * 3,
        out_specs=vmem,
        scratch_shapes=[
            pltpu.VMEM((blocks, BLK, 256), BF16),
            pltpu.VMEM((blocks, 80, BLK), BF16),
            pltpu.VMEM((BLK, 256), BF16),
            pltpu.VMEM((80, BLK), F32),
            pltpu.VMEM((1, BLK), F32),
            pltpu.SMEM((blocks,), F32),
        ],
        compiler_params=pltpu.CompilerParams(vmem_limit_bytes=48 * 1024 * 1024),
        name="attention",
    )(q, kvx, gain)


MESH = pl.DeviceIdType.MESH
GROUP = 4


def experts_kernel(
    out_ref, wg_hbm, wu_hbm, wd_hbm, ret_ref,
    x, p, r_in, m_in, wg, wu, wd,
    w_sem, a2a_send, a2a_recv, ag_send, ag_recv, relay_send, relay_recv,
    r_send, r_recv, m_send, m_recv, ret_send, ret_recv,
):
    experts, slots, width = out_ref.shape
    tps = x.shape[0]
    steps = experts // GROUP
    half = GROUP // 2
    s = lax.axis_index("sp")
    t = lax.axis_index("tp")
    right = lax.rem(t + 1, tps)
    left = lax.rem(t + tps - 1, tps)
    far = lax.rem(t + 2, tps)
    sides = (right, left)

    loads = [
        pltpu.make_async_copy(a.at[0], b, w_sem.at[i])
        for i, (a, b) in enumerate(((wg_hbm, wg), (wu_hbm, wu), (wd_hbm, wd)))
    ]
    for load in loads:
        load.start()

    barrier = pltpu.get_barrier_semaphore()

    @pl.loop(1, experts)
    def _(k):
        pl.semaphore_signal(
            barrier, 1, device_id=(lax.rem(s + k, experts), t), device_id_type=MESH
        )

    for side in sides:
        pl.semaphore_signal(barrier, 1, device_id=(s, side), device_id_type=MESH)
    pl.semaphore_wait(barrier, experts - 1 + 2)

    def send(src, dst, send_sem, recv_sem, sp, tp):
        return pltpu.make_async_remote_copy(
            src_ref=src,
            dst_ref=dst,
            send_sem=send_sem,
            recv_sem=recv_sem,
            device_id=(sp, tp),
            device_id_type=MESH,
        )

    def to_side(i, src, dst, send_sem, recv_sem):
        return send(src, dst, send_sem, recv_sem, s, sides[i])

    @pl.loop(1, experts)
    def _(k):
        to = lax.rem(s + k, experts)
        send(out_ref.at[to], x.at[t, k], a2a_send, a2a_recv.at[k // GROUP], to, t).start()

    x[t, 0] = out_ref[s]

    def whole(c):
        return pl.ds(c * GROUP, GROUP)

    def part(c, i):
        return pl.ds(c * GROUP + i * half, half)

    def enter(c):
        @pl.when(c == 0)
        def _():
            first = x.at[t, pl.ds(1, GROUP - 1)]
            send(first, first, a2a_send, a2a_recv.at[0], s, right).wait_recv()

        @pl.when(c > 0)
        def _():
            rows = x.at[t, whole(c)]
            send(rows, rows, a2a_send, a2a_recv.at[c], s, right).wait_recv()

        rows = x.at[t, whole(c)]
        for i in range(2):
            to_side(i, rows, rows, ag_send.at[i], ag_recv.at[i, c]).start()

    def relay(c):
        for i in range(2):
            origin = sides[1 - i]
            rows = x.at[origin, whole(c)]
            to_side(i, rows, rows, ag_send.at[i], ag_recv.at[i, c]).wait_recv()
            rows = x.at[origin, part(c, i)]
            to_side(i, rows, rows, relay_send.at[i], relay_recv.at[i, c]).start()

    def compute(c):
        for i in range(2):
            rows = x.at[far, part(c, i)]
            to_side(i, rows, rows, relay_send.at[i], relay_recv.at[i, c]).wait_recv()
        rows = x[:, whole(c)].reshape(tps * GROUP * slots, width)
        gate = jnp.dot(rows, wg[...], preferred_element_type=F32)
        up = jnp.dot(rows, wu[...], preferred_element_type=F32)
        hidden = (gate / (1.0 + jnp.exp(-gate)) * up).astype(BF16)
        made = jnp.dot(hidden, wd[...], preferred_element_type=F32)
        p[:, whole(c)] = made.astype(BF16).reshape(tps, GROUP, slots, width)
        for i in range(2):
            to_side(
                i, p.at[far, part(c, i)], r_in.at[i, pl.ds(c * half, half)],
                r_send.at[i], r_recv.at[i, c],
            ).start()

    def pass_on(c):
        for i in range(2):
            got = r_in.at[i, pl.ds(c * half, half)]
            to_side(i, got, got, r_send.at[i], r_recv.at[i, c]).wait_recv()
            mine = p[sides[i], part(c, i)].astype(F32)
            p[sides[i], part(c, i)] = (mine + got[...].astype(F32)).astype(BF16)
        for i in range(2):
            to_side(
                i, p.at[sides[i], whole(c)], m_in.at[i, whole(c)], m_send.at[i], m_recv.at[i, c]
            ).start()

    def leave(c):
        total = p[t, whole(c)].astype(F32)
        for i in range(2):
            got = m_in.at[i, whole(c)]
            to_side(i, got, got, m_send.at[i], m_recv.at[i, c]).wait_recv()
            total = total + got[...].astype(F32)
        p[t, whole(c)] = total.astype(BF16)

        @pl.when(c == 0)
        def _():
            ret_ref[s] = p[t, 0]

        @pl.loop(jnp.where(c == 0, 1, 0), GROUP)
        def _(j):
            k = c * GROUP + j
            to = lax.rem(s + experts - k, experts)
            send(p.at[t, k], ret_ref.at[s], ret_send, ret_recv, to, t).start()

    @pl.loop(0, steps + 4)
    def _(i):
        @pl.when(i < steps)
        def _():
            enter(i)

        @pl.when((i >= 1) & (i < steps + 1))
        def _():
            relay(i - 1)

        @pl.when(i >= 4)
        def _():
            leave(i - 4)

        @pl.when((i >= 3) & (i < steps + 3))
        def _():
            pass_on(i - 3)

        @pl.when(i == 2)
        def _():
            for load in loads:
                load.wait()

        @pl.when((i >= 2) & (i < steps + 2))
        def _():
            compute(i - 2)

    most = x.at[0, pl.ds(0, experts - 1)]
    every = x.at[0]
    some = x.at[0, pl.ds(0, experts // 2)]
    back = ret_ref.at[pl.ds(0, experts - 1)]
    send(most, back, a2a_send, ret_recv, s, right).wait_send()
    send(most, back, ret_send, ret_recv, s, right).wait()
    for i in range(2):
        to_side(i, every, every, ag_send.at[i], ag_recv.at[i, 0]).wait_send()
        to_side(i, some, some, relay_send.at[i], relay_recv.at[i, 0]).wait_send()
        to_side(i, some, some, r_send.at[i], r_recv.at[i, 0]).wait_send()
        to_side(i, every, every, m_send.at[i], m_recv.at[i, 0]).wait_send()


def at_experts(outbound, w_gate, w_up, w_down):
    experts, slots, width = outbound.shape
    hidden = w_gate.shape[2]
    tps = lax.axis_size("tp")
    steps = experts // GROUP
    vmem = pl.BlockSpec(memory_space=pltpu.VMEM)
    hbm = pl.BlockSpec(memory_space=pl.ANY)
    dma = pltpu.SemaphoreType.DMA
    return pl.pallas_call(
        experts_kernel,
        out_shape=jax.ShapeDtypeStruct(outbound.shape, BF16),
        in_specs=[vmem, hbm, hbm, hbm],
        out_specs=vmem,
        scratch_shapes=[
            pltpu.VMEM((tps, experts, slots, width), BF16),
            pltpu.VMEM((tps, experts, slots, width), BF16),
            pltpu.VMEM((2, experts // 2, slots, width), BF16),
            pltpu.VMEM((2, experts, slots, width), BF16),
            pltpu.VMEM((width, hidden), BF16),
            pltpu.VMEM((width, hidden), BF16),
            pltpu.VMEM((hidden, width), BF16),
            dma((3,)),
            dma,
            dma((steps,)),
            dma((2,)),
            dma((2, steps)),
            dma((2,)),
            dma((2, steps)),
            dma((2,)),
            dma((2, steps)),
            dma((2,)),
            dma((2, steps)),
            dma,
            dma,
        ],
        compiler_params=pltpu.CompilerParams(
            collective_id=1, has_side_effects=True, vmem_limit_bytes=58 * 1024 * 1024
        ),
        name="experts",
    )(outbound, w_gate, w_up, w_down)


def on_device(
    queries,
    keys,
    values,
    cum_gate,
    documents,
    head_gain,
    out_weight,
    resid,
    norm_gain,
    routes,
    route_weights,
    w_gate,
    w_up,
    w_down,
):
    tokens = queries.shape[0]
    heads = cum_gate.shape[1]
    sp_count = lax.axis_size("sp")
    members = sp_count // heads
    z = lax.axis_index("sp") // members

    def by_head(a):
        return a.reshape(tokens, heads, 64).transpose(1, 0, 2)

    qh = by_head(queries)
    q_pack = jnp.concatenate([qh[:, : BLK // 2], qh[:, BLK // 2 :]], axis=-1)
    kv = jnp.concatenate([by_head(keys), by_head(values)], axis=-1)
    gate = cum_gate.T
    gate0 = gate[:, :1]
    rel = jnp.stack(pieces_of((gate0 - gate) * LOG2E), axis=1).reshape(heads, 12, 128)
    docs = jnp.broadcast_to(documents.astype(F32).reshape(1, 4, 128), (heads, 4, 128))
    zero_row = jnp.pad(jnp.stack(pieces_of(gate0), axis=2), ((0, 0), (0, 15), (0, 125)))
    extra = jnp.concatenate([rel, docs, zero_row], axis=1).astype(BF16)
    payload = jnp.concatenate([kv, extra, q_pack], axis=1)
    columns = [[j + members * g for g in range(heads)] for j in range(members)]
    rows = [[j + members * g for j in range(members)] for g in range(heads)]
    arrived = lax.all_to_all(
        payload, "sp", split_axis=0, concat_axis=0, axis_index_groups=columns, tiled=True
    )
    kvx = lax.all_gather(arrived[:, : BLK + EXTRA], "sp", axis=0, axis_index_groups=rows)
    gain = jnp.broadcast_to(lax.dynamic_slice_in_dim(head_gain, z * 64, 64)[:, None], (64, 128))
    normed = attend(arrived[:, BLK + EXTRA :], kvx, gain)
    normed = lax.all_to_all(
        normed, "sp", split_axis=0, concat_axis=0, axis_index_groups=columns, tiled=True
    ).reshape(heads * 64, tokens)
    tp_count = lax.axis_size("tp")
    local_rows = tokens // tp_count
    regrouped = lax.all_to_all(normed, "tp", split_axis=1, concat_axis=0, tiled=True)
    projected = lax.dot_general(
        regrouped, out_weight, (((0,), (0,)), ((), ())), preferred_element_type=F32
    )
    stream = lax.optimization_barrier((resid.astype(F32) + projected).astype(BF16))
    widened = stream.astype(F32)
    mean_wide = jnp.mean(widened * widened, axis=-1, keepdims=True)
    expert_input = (widened * lax.rsqrt(mean_wide + EPS) * norm_gain).astype(BF16)
    top_count = routes.shape[1]
    expert_count = sp_count
    model_width = stream.shape[1]
    capacity = 2 * top_count * tokens // (tp_count * expert_count)
    flat_routes = routes.reshape(-1)
    route_total = flat_routes.shape[0]
    onehot = (flat_routes[:, None] == jnp.arange(expert_count, dtype=jnp.int32)[None, :]).astype(
        jnp.int32
    )
    ranks = jnp.sum(jnp.cumsum(onehot, axis=0) * onehot, axis=1) - 1
    targets = flat_routes * capacity + ranks
    owners = jnp.arange(route_total, dtype=jnp.int32) // top_count
    slot_owner = jnp.zeros((expert_count * capacity,), jnp.int32).at[targets].set(owners)
    slot_used = jnp.zeros((expert_count * capacity,), jnp.bool_).at[targets].set(True)
    outbound = jnp.where(slot_used[:, None], expert_input[slot_owner], jnp.zeros((), BF16))
    outbound = outbound.reshape(expert_count, capacity, model_width)

    returned = at_experts(outbound, w_gate, w_up, w_down)
    results = returned.reshape(expert_count * capacity, model_width)[targets]
    results = results.reshape(local_rows, top_count, model_width)
    mixed = widened + jnp.sum(route_weights[:, :, None] * results.astype(F32), axis=1)
    return mixed.astype(BF16)


def solution(mesh):
    in_specs = (
        P("sp", "tp"),
        P("sp", "tp"),
        P("sp", "tp"),
        P("sp", "tp"),
        P("sp"),
        P("tp"),
        P(),
        P(("sp", "tp"), None),
        P(),
        P(("sp", "tp"), None),
        P(("sp", "tp"), None),
        P("sp", None, "tp"),
        P("sp", None, "tp"),
        P("sp", "tp", None),
    )
    out_specs = P(("sp", "tp"), None)
    return jax.shard_map(
        on_device, mesh=mesh, in_specs=in_specs, out_specs=out_specs, check_vma=False
    )
```

```python
import jax
import jax.numpy as jnp
from jax import lax
from jax.experimental import pallas as pl
from jax.experimental.pallas import tpu as pltpu
from jax.sharding import PartitionSpec as P

EPS = 1e-06
LOG2E = 1.4426950408889634
BLK = 512
EXTRA = 32
NEG = -1e30
F32 = jnp.float32
BF16 = jnp.bfloat16


def pieces_of(x):
    hi = lax.reduce_precision(x, 8, 7)
    rest = x - hi
    mid = lax.reduce_precision(rest, 8, 7)
    return hi, mid, rest - mid


def attention_kernel(q_ref, kvx_ref, gain_ref, o_ref, kp, vt, qp, acc, mrow, g0):
    members = kvx_ref.shape[0]
    groups = kvx_ref.shape[1]
    blocks = members * groups
    me = lax.rem(lax.axis_index("sp"), members)
    lane = lax.broadcasted_iota(jnp.int32, (128, 128), 1)
    lane_wide = lax.broadcasted_iota(jnp.int32, (BLK, 128), 1)
    row_extra = lax.broadcasted_iota(jnp.int32, (EXTRA, 128), 0)
    is_doc = (row_extra >= 12) & (row_extra < 16)

    def prepare(kb, counts):
        member, group = lax.rem(kb, members), kb // members
        extra = kvx_ref[member, group, BLK : BLK + EXTRA, :].astype(F32)
        g0[kb] = jnp.sum(jnp.where(row_extra == 16, extra, 0.0))
        counts = tuple(
            count + jnp.where(is_doc & (extra < d + 0.5), 1.0, 0.0)
            for d, count in enumerate(counts)
        )
        turned = jnp.concatenate([extra, jnp.zeros((128 - EXTRA, 128), F32)], axis=0).T
        for c in range(4):
            kp[kb, c * 128 : (c + 1) * 128, 128:256] = jnp.where(
                (lane < 12) & (lane % 4 == c), turned, 0.0
            ).astype(BF16)
        kv = kvx_ref[member, group, 0:BLK, :].astype(F32)
        kp[kb, :, 0:128] = jnp.where(lane_wide < 64, kv, pltpu.roll(kv, 64, 1)).astype(BF16)
        vt[kb, 16:80, :] = kv.T[64:128, :].astype(BF16)
        vt[kb, 0:16, :] = jnp.ones((16, BLK), BF16)
        return counts

    zero = jnp.zeros((EXTRA, 128), F32)
    counts = lax.fori_loop(0, blocks, prepare, (zero, zero, zero))
    starts = [jnp.sum(c).astype(jnp.int32) for c in counts]

    def one_query_block(i, unused):
        qb = i * members + me
        half = q_ref[i].astype(F32) * (LOG2E * 0.125)
        q = jnp.concatenate([half, pltpu.roll(half, 64, 1)], axis=0)
        hi = q.astype(BF16).astype(F32)
        low = pltpu.roll(q - hi, 64, 1)
        qp[:, 0:128] = jnp.where(lane_wide < 64, hi, low).astype(BF16)
        qp[:, 128:256] = jnp.where(lane_wide < 12, 1.0, 0.0).astype(BF16)
        extra = kvx_ref[me, i, BLK : BLK + EXTRA, :].astype(F32)
        doc = jnp.concatenate([extra[12 + c : 13 + c, :] for c in range(4)], axis=1)
        start = jnp.where(
            doc < 0.5,
            0,
            jnp.where(doc < 1.5, starts[0], jnp.where(doc < 2.5, starts[1], starts[2])),
        )
        first = jnp.min(start)
        last = jnp.max(start)
        base = g0[qb]

        def visit(kb, masked, fresh):
            shift = (base - g0[kb]) * LOG2E
            scores = lax.dot_general(
                kp[kb], qp[...], (((1,), (1,)), ((), ())), preferred_element_type=F32
            )
            if masked:
                key_pos = kb * BLK + lax.broadcasted_iota(jnp.int32, (BLK, BLK), 0)
                query_pos = qb * BLK + lax.broadcasted_iota(jnp.int32, (BLK, BLK), 1)
                allowed = (key_pos <= query_pos) & (key_pos >= start)
                scores = jnp.where(allowed, scores, NEG)
            top = jnp.max(scores, axis=0, keepdims=True) + shift
            if not fresh:
                old = mrow[...]
                top = jnp.maximum(old, top)
            weights = jnp.exp2(scores - (top - shift)).astype(BF16)
            added = jnp.dot(vt[kb], weights, preferred_element_type=F32)
            if fresh:
                acc[...] = added
            else:
                acc[...] = acc[...] * jnp.exp2(old - top) + added
            mrow[...] = top

        visit(qb, True, True)

        def earlier(kb, carry):
            plain = kb * BLK >= last

            @pl.when(plain)
            def _():
                visit(kb, False, False)

            @pl.when(jnp.logical_not(plain))
            def _():
                visit(kb, True, False)

            return carry

        lax.fori_loop(first // BLK, qb, earlier, 0)
        out = acc[16:80, :] / acc[0:1, :]
        mean_square = jnp.mean(out * out, axis=0, keepdims=True)
        gain = jnp.concatenate([gain_ref[...]] * 4, axis=1)
        normed = (out * lax.rsqrt(mean_square + EPS) * gain).astype(BF16)
        for c in range(4):
            o_ref[i, c] = normed[:, c * 128 : (c + 1) * 128]
        return unused

    lax.fori_loop(0, groups, one_query_block, 0)


def attend(q, kvx, gain):
    members, groups = kvx.shape[:2]
    blocks = members * groups
    vmem = pl.BlockSpec(memory_space=pltpu.VMEM)
    return pl.pallas_call(
        attention_kernel,
        out_shape=jax.ShapeDtypeStruct((groups, 4, 64, 128), BF16),
        in_specs=[vmem] * 3,
        out_specs=vmem,
        scratch_shapes=[
            pltpu.VMEM((blocks, BLK, 256), BF16),
            pltpu.VMEM((blocks, 80, BLK), BF16),
            pltpu.VMEM((BLK, 256), BF16),
            pltpu.VMEM((80, BLK), F32),
            pltpu.VMEM((1, BLK), F32),
            pltpu.SMEM((blocks,), F32),
        ],
        compiler_params=pltpu.CompilerParams(vmem_limit_bytes=48 * 1024 * 1024),
        name="attention",
    )(q, kvx, gain)


MESH = pl.DeviceIdType.MESH
GROUP = 4
KVX = BLK + EXTRA


def remote(src, dst, send_sem, recv_sem, sp, tp):
    return pltpu.make_async_remote_copy(
        src_ref=src,
        dst_ref=dst,
        send_sem=send_sem,
        recv_sem=recv_sem,
        device_id=(sp, tp),
        device_id_type=MESH,
    )


def gather_kernel(
    pay_ref, q_ref, kvx_ref, q_send, q_recv, a_send, a_recv, y_send, y_recv,
    h_send, h_recv, d_send, d_recv,
):
    members, groups = kvx_ref.shape[:2]
    ring = members // 2
    s = lax.axis_index("sp")
    t = lax.axis_index("tp")
    z, j = s // members, lax.rem(s, members)
    y, core = j // 2, lax.rem(j, 2)

    def member(dy, other=0):
        c = 1 - core if other else core
        return lax.rem(y + dy + ring, ring) * 2 + c

    sides = (member(1), member(-1))
    far = member(2)
    peers = [lax.rem(z + d, groups) * members + j for d in range(1, groups)]
    peers += [z * members + m for m in (*sides, member(0, 1))]
    barrier = pltpu.get_barrier_semaphore()
    for peer in peers:
        pl.semaphore_signal(barrier, 1, device_id=(peer, t), device_id_type=MESH)
    pl.semaphore_wait(barrier, len(peers))

    order = (0, 1, 3, 2)

    def kv_copy(n, d, source):
        to = lax.rem(z + d, groups)
        return remote(
            pay_ref.at[to, pl.ds(0, KVX)], kvx_ref.at[j, source], a_send, a_recv.at[n],
            to * members + j, t,
        )

    def q_copy(n, d, source):
        to = lax.rem(z + d, groups)
        return remote(
            pay_ref.at[to, pl.ds(KVX, BLK // 2)], q_ref.at[source], q_send, q_recv.at[n],
            to * members + j, t,
        )

    for n, d in enumerate(order):
        if d:
            kv_copy(n, d, z).start()
    for n, d in enumerate(order):
        if d:
            q_copy(n, d, z).start()
    kvx_ref[j, z] = pay_ref[z, 0:KVX, :]
    q_ref[z] = pay_ref[z, KVX : KVX + BLK // 2, :]

    def source_of(n):
        return lax.rem(z - order[n] + groups, groups)

    def to_side(i, rows, send_sem, recv_sem):
        return remote(rows, rows, send_sem, recv_sem, z * members + sides[i], t)

    def to_core(kind, n, m):
        rows = kvx_ref.at[m, source_of(n)]
        return remote(
            rows, rows, d_send, d_recv.at[kind, n], z * members + member(0, 1), t
        )

    def piece(i):
        return pl.ds(i * (KVX // 2), KVX // 2)

    def enter(n):
        if n:
            kv_copy(n, order[n], source_of(n)).wait_recv()
        rows = kvx_ref.at[j, source_of(n)]
        for i in range(2):
            to_side(i, rows, y_send.at[i], y_recv.at[i, n]).start()
        to_core(0, n, j).start()

    def relay(n):
        for i in range(2):
            origin = sides[1 - i]
            rows = kvx_ref.at[origin, source_of(n)]
            to_side(i, rows, y_send.at[i], y_recv.at[i, n]).wait_recv()
            rows = kvx_ref.at[origin, source_of(n), piece(i)]
            to_side(i, rows, h_send.at[i], h_recv.at[i, n]).start()
            to_core(1 + i, n, origin).start()

    def finish(n):
        for i in range(2):
            rows = kvx_ref.at[far, source_of(n), piece(i)]
            to_side(i, rows, h_send.at[i], h_recv.at[i, n]).wait_recv()
        to_core(3, n, far).start()

    for step in range(groups + 2):
        if step < groups:
            enter(step)
        if 1 <= step <= groups:
            relay(step - 1)
        if step >= 2:
            finish(step - 2)
    for n in range(groups):
        for kind in range(4):
            to_core(kind, n, member((0, -1, 1, 2)[kind], 1)).wait_recv()
    for n in range(1, groups):
        q_copy(n, order[n], source_of(n)).wait_recv()
    for n in range(1, groups):
        kv_copy(n, order[n], z).wait_send()
        q_copy(n, order[n], z).wait_send()
    rows = kvx_ref.at[j]
    halves = kvx_ref.at[0, :, pl.ds(0, KVX // 2)]
    for i in range(2):
        to_side(i, rows, y_send.at[i], y_recv.at[i, 0]).wait_send()
        to_side(i, halves, h_send.at[i], h_recv.at[i, 0]).wait_send()
    every = kvx_ref.at[pl.ds(0, 4)]
    remote(every, every, d_send, d_recv.at[0, 0], z * members, t).wait_send()


def gather_history(payload, members):
    groups = payload.shape[0]
    vmem = pl.BlockSpec(memory_space=pltpu.VMEM)
    dma = pltpu.SemaphoreType.DMA
    return pl.pallas_call(
        gather_kernel,
        out_shape=(
            jax.ShapeDtypeStruct((groups, BLK // 2, 128), BF16),
            jax.ShapeDtypeStruct((members, groups, KVX, 128), BF16),
        ),
        in_specs=[vmem],
        out_specs=(vmem, vmem),
        scratch_shapes=[
            dma,
            dma((groups,)),
            dma,
            dma((groups,)),
            dma((2,)),
            dma((2, groups)),
            dma((2,)),
            dma((2, groups)),
            dma,
            dma((4, groups)),
        ],
        compiler_params=pltpu.CompilerParams(
            collective_id=0, has_side_effects=True, vmem_limit_bytes=16 * 1024 * 1024
        ),
        name="gather_history",
    )(payload)


def experts_kernel(
    normed_ref, ow_hbm, resid_ref, ng_ref, rows_ref, cols_ref, rw_ref, wg_hbm, wu_hbm, wd_hbm,
    mixed_ref,
    heads, ow, stream, out_ref, ret_ref, x, p, r_in, m_in, wg, wu, wd,
    w_sem, head_send, head_recv, a2a_send, a2a_recv, ag_send, ag_recv, relay_send, relay_recv,
    r_send, r_recv, m_send, m_recv, ret_send, ret_recv,
):
    experts, slots, width = out_ref.shape
    groups = normed_ref.shape[0]
    tps = x.shape[0]
    members = experts // groups
    steps = experts // GROUP
    half = GROUP // 2
    send = remote
    s = lax.axis_index("sp")
    t = lax.axis_index("tp")
    z, j = s // members, lax.rem(s, members)
    right = lax.rem(t + 1, tps)
    left = lax.rem(t + tps - 1, tps)
    far = lax.rem(t + 2, tps)
    sides = (right, left)

    loads = [
        pltpu.make_async_copy(a, b, w_sem.at[i])
        for i, (a, b) in enumerate(
            ((ow_hbm, ow), (wg_hbm.at[0], wg), (wu_hbm.at[0], wu), (wd_hbm.at[0], wd))
        )
    ]
    for load in loads:
        load.start()

    barrier = pltpu.get_barrier_semaphore()

    @pl.loop(1, experts)
    def _(k):
        pl.semaphore_signal(
            barrier, 1, device_id=(lax.rem(s + k, experts), t), device_id_type=MESH
        )

    for side in sides:
        pl.semaphore_signal(barrier, 1, device_id=(s, side), device_id_type=MESH)

    def owner(n):
        return lax.rem(z + n // tps, groups), lax.rem(t + lax.rem(n, tps), tps)

    @pl.loop(1, groups * tps)
    def _(n):
        zz, tt = owner(n)
        pl.semaphore_signal(barrier, 1, device_id=(zz * members + j, tt), device_id_type=MESH)

    pl.semaphore_wait(barrier, experts - 1 + 2 + groups * tps - 1)

    mine = t * groups + z

    @pl.loop(1, groups * tps)
    def _(n):
        zz, tt = owner(n)
        send(
            normed_ref.at[zz, tt], heads.at[mine], head_send, head_recv, zz * members + j, tt
        ).start()

    heads[mine] = normed_ref[z, t]
    slot_ids = lax.broadcasted_iota(jnp.int32, (experts * slots, 128), 0)
    chosen = (slot_ids == rows_ref[0:1, :]) | (slot_ids == rows_ref[1:2, :])
    chosen = jnp.where(chosen, 1.0, 0.0).astype(BF16)
    loads[0].wait()
    others = heads.at[pl.ds(0, groups * tps - 1)]
    send(others, others, head_send, head_recv, s, right).wait()
    projected = lax.dot_general(
        heads[...].reshape(groups * tps * 64, 128), ow[...], (((0,), (0,)), ((), ())),
        preferred_element_type=F32,
    )
    stream[...] = (resid_ref[...].astype(F32) + projected).astype(BF16)
    widened = stream[...].astype(F32)
    mean_wide = jnp.mean(widened * widened, axis=-1, keepdims=True)
    expert_input = (widened * lax.rsqrt(mean_wide + EPS) * ng_ref[...]).astype(BF16)
    out_ref[...] = (
        jnp.dot(chosen, expert_input, preferred_element_type=F32)
        .astype(BF16)
        .reshape(experts, slots, width)
    )

    def to_side(i, src, dst, send_sem, recv_sem):
        return send(src, dst, send_sem, recv_sem, s, sides[i])

    @pl.loop(1, experts)
    def _(k):
        to = lax.rem(s + k, experts)
        send(out_ref.at[to], x.at[t, k], a2a_send, a2a_recv.at[k // GROUP], to, t).start()

    x[t, 0] = out_ref[s]

    def whole(c):
        return pl.ds(c * GROUP, GROUP)

    def part(c, i):
        return pl.ds(c * GROUP + i * half, half)

    def enter(c):
        @pl.when(c == 0)
        def _():
            first = x.at[t, pl.ds(1, GROUP - 1)]
            send(first, first, a2a_send, a2a_recv.at[0], s, right).wait_recv()

        @pl.when(c > 0)
        def _():
            rows = x.at[t, whole(c)]
            send(rows, rows, a2a_send, a2a_recv.at[c], s, right).wait_recv()

        rows = x.at[t, whole(c)]
        for i in range(2):
            to_side(i, rows, rows, ag_send.at[i], ag_recv.at[i, c]).start()

    def relay(c):
        for i in range(2):
            origin = sides[1 - i]
            rows = x.at[origin, whole(c)]
            to_side(i, rows, rows, ag_send.at[i], ag_recv.at[i, c]).wait_recv()
            rows = x.at[origin, part(c, i)]
            to_side(i, rows, rows, relay_send.at[i], relay_recv.at[i, c]).start()

    def compute(c):
        for i in range(2):
            rows = x.at[far, part(c, i)]
            to_side(i, rows, rows, relay_send.at[i], relay_recv.at[i, c]).wait_recv()
        rows = x[:, whole(c)].reshape(tps * GROUP * slots, width)
        gate = jnp.dot(rows, wg[...], preferred_element_type=F32)
        up = jnp.dot(rows, wu[...], preferred_element_type=F32)
        hidden = (gate / (1.0 + jnp.exp(-gate)) * up).astype(BF16)
        made = jnp.dot(hidden, wd[...], preferred_element_type=F32)
        p[:, whole(c)] = made.astype(BF16).reshape(tps, GROUP, slots, width)
        for i in range(2):
            to_side(
                i, p.at[far, part(c, i)], r_in.at[i, pl.ds(c * half, half)],
                r_send.at[i], r_recv.at[i, c],
            ).start()

    def pass_on(c):
        for i in range(2):
            got = r_in.at[i, pl.ds(c * half, half)]
            to_side(i, got, got, r_send.at[i], r_recv.at[i, c]).wait_recv()
            mine = p[sides[i], part(c, i)].astype(F32)
            p[sides[i], part(c, i)] = (mine + got[...].astype(F32)).astype(BF16)
        for i in range(2):
            to_side(
                i, p.at[sides[i], whole(c)], m_in.at[i, whole(c)], m_send.at[i], m_recv.at[i, c]
            ).start()

    def leave(c):
        total = p[t, whole(c)].astype(F32)
        for i in range(2):
            got = m_in.at[i, whole(c)]
            to_side(i, got, got, m_send.at[i], m_recv.at[i, c]).wait_recv()
            total = total + got[...].astype(F32)
        p[t, whole(c)] = total.astype(BF16)

        @pl.when(c == 0)
        def _():
            ret_ref[s] = p[t, 0]

        @pl.loop(jnp.where(c == 0, 1, 0), GROUP)
        def _(j):
            k = c * GROUP + j
            to = lax.rem(s + experts - k, experts)
            send(p.at[t, k], ret_ref.at[s], ret_send, ret_recv, to, t).start()

    @pl.loop(0, steps + 4)
    def _(i):
        @pl.when(i < steps)
        def _():
            enter(i)

        @pl.when((i >= 1) & (i < steps + 1))
        def _():
            relay(i - 1)

        @pl.when(i >= 4)
        def _():
            leave(i - 4)

        @pl.when((i >= 3) & (i < steps + 3))
        def _():
            pass_on(i - 3)

        @pl.when(i == 2)
        def _():
            for load in loads[1:]:
                load.wait()

        @pl.when((i >= 2) & (i < steps + 2))
        def _():
            compute(i - 2)

    most = x.at[0, pl.ds(0, experts - 1)]
    every = x.at[0]
    some = x.at[0, pl.ds(0, experts // 2)]
    back = ret_ref.at[pl.ds(0, experts - 1)]
    send(most, back, a2a_send, ret_recv, s, right).wait_send()
    send(most, back, ret_send, ret_recv, s, right).wait()
    for i in range(2):
        to_side(i, every, every, ag_send.at[i], ag_recv.at[i, 0]).wait_send()
        to_side(i, some, some, relay_send.at[i], relay_recv.at[i, 0]).wait_send()
        to_side(i, some, some, r_send.at[i], r_recv.at[i, 0]).wait_send()
        to_side(i, every, every, m_send.at[i], m_recv.at[i, 0]).wait_send()
    lanes = lax.broadcasted_iota(jnp.int32, (128, experts * slots), 1)
    spread = jnp.where(lanes == cols_ref[:, 0:1], rw_ref[:, 0:1], 0.0) + jnp.where(
        lanes == cols_ref[:, 1:2], rw_ref[:, 1:2], 0.0
    )
    results = ret_ref[...].reshape(experts * slots, width)
    mixed = stream[...].astype(F32)
    for _ in range(3):
        digit = spread.astype(BF16)
        mixed = mixed + jnp.dot(digit, results, preferred_element_type=F32)
        spread = spread - digit.astype(F32)
    mixed_ref[...] = mixed.astype(BF16)


def at_experts(normed, out_weight, resid, norm_gain, targets, route_weights, w_gate, w_up, w_down):
    groups, tps = normed.shape[:2]
    rows, width = resid.shape
    hidden = w_gate.shape[2]
    experts = lax.axis_size("sp")
    slots = 16
    steps = experts // GROUP
    vmem = pl.BlockSpec(memory_space=pltpu.VMEM)
    hbm = pl.BlockSpec(memory_space=pl.ANY)
    dma = pltpu.SemaphoreType.DMA
    return pl.pallas_call(
        experts_kernel,
        out_shape=jax.ShapeDtypeStruct((rows, width), BF16),
        in_specs=[vmem, hbm, vmem, vmem, vmem, vmem, vmem, hbm, hbm, hbm],
        out_specs=vmem,
        scratch_shapes=[
            pltpu.VMEM((groups * tps, 64, 128), BF16),
            pltpu.VMEM(out_weight.shape, BF16),
            pltpu.VMEM((rows, width), BF16),
            pltpu.VMEM((experts, slots, width), BF16),
            pltpu.VMEM((experts, slots, width), BF16),
            pltpu.VMEM((tps, experts, slots, width), BF16),
            pltpu.VMEM((tps, experts, slots, width), BF16),
            pltpu.VMEM((2, experts // 2, slots, width), BF16),
            pltpu.VMEM((2, experts, slots, width), BF16),
            pltpu.VMEM((width, hidden), BF16),
            pltpu.VMEM((width, hidden), BF16),
            pltpu.VMEM((hidden, width), BF16),
            dma((4,)),
            dma,
            dma,
            dma,
            dma((steps,)),
            dma((2,)),
            dma((2, steps)),
            dma((2,)),
            dma((2, steps)),
            dma((2,)),
            dma((2, steps)),
            dma((2,)),
            dma((2, steps)),
            dma,
            dma,
        ],
        compiler_params=pltpu.CompilerParams(
            collective_id=1, has_side_effects=True, vmem_limit_bytes=60 * 1024 * 1024
        ),
        name="experts",
    )(
        normed, out_weight, resid, norm_gain.reshape(1, width), targets.T, targets, route_weights,
        w_gate, w_up, w_down,
    )


def on_device(
    queries,
    keys,
    values,
    cum_gate,
    documents,
    head_gain,
    out_weight,
    resid,
    norm_gain,
    routes,
    route_weights,
    w_gate,
    w_up,
    w_down,
):
    tokens = queries.shape[0]
    heads = cum_gate.shape[1]
    sp_count = lax.axis_size("sp")
    members = sp_count // heads
    z = lax.axis_index("sp") // members

    def by_head(a):
        return a.reshape(tokens, heads, 64).transpose(1, 0, 2)

    qh = by_head(queries)
    q_pack = jnp.concatenate([qh[:, : BLK // 2], qh[:, BLK // 2 :]], axis=-1)
    kv = jnp.concatenate([by_head(keys), by_head(values)], axis=-1)
    gate = cum_gate.T
    gate0 = gate[:, :1]
    rel = jnp.stack(pieces_of((gate0 - gate) * LOG2E), axis=1).reshape(heads, 12, 128)
    docs = jnp.broadcast_to(documents.astype(F32).reshape(1, 4, 128), (heads, 4, 128))
    zero_row = jnp.pad(jnp.stack(pieces_of(gate0), axis=2), ((0, 0), (0, 15), (0, 125)))
    extra = jnp.concatenate([rel, docs, zero_row], axis=1).astype(BF16)
    payload = jnp.concatenate([kv, extra, q_pack], axis=1)
    q, kvx = gather_history(payload, members)
    gain = jnp.broadcast_to(lax.dynamic_slice_in_dim(head_gain, z * 64, 64)[:, None], (64, 128))
    normed = attend(q, kvx, gain)
    flat_routes = routes.reshape(-1)
    onehot = (flat_routes[:, None] == jnp.arange(sp_count, dtype=jnp.int32)[None, :]).astype(
        jnp.int32
    )
    ranks = jnp.sum(jnp.cumsum(onehot, axis=0) * onehot, axis=1) - 1
    targets = (flat_routes * 16 + ranks).reshape(routes.shape)
    return at_experts(
        normed, out_weight, resid, norm_gain, targets, route_weights, w_gate, w_up, w_down
    )


def solution(mesh):
    in_specs = (
        P("sp", "tp"),
        P("sp", "tp"),
        P("sp", "tp"),
        P("sp", "tp"),
        P("sp"),
        P("tp"),
        P(),
        P(("sp", "tp"), None),
        P(),
        P(("sp", "tp"), None),
        P(("sp", "tp"), None),
        P("sp", None, "tp"),
        P("sp", None, "tp"),
        P("sp", "tp", None),
    )
    out_specs = P(("sp", "tp"), None)
    return jax.shard_map(
        on_device, mesh=mesh, in_specs=in_specs, out_specs=out_specs, check_vma=False
    )
```

```python
import jax
import jax.numpy as jnp
from jax import lax
from jax.experimental import pallas as pl
from jax.experimental.pallas import tpu as pltpu
from jax.sharding import PartitionSpec as P

EPS = 1e-06
LOG2E = 1.4426950408889634
BLK = 512
EXTRA = 32
NEG = -1e30
F32 = jnp.float32
BF16 = jnp.bfloat16


def pieces_of(x):
    hi = x.astype(BF16).astype(F32)
    rest = x - hi
    mid = rest.astype(BF16).astype(F32)
    return hi, mid, rest - mid


def pack(queries_ref, keys_ref, values_ref, gate_ref, doc_ref, pay_ref):
    lane = lax.broadcasted_iota(jnp.int32, (BLK, 128), 1)
    half = lane[: BLK // 2]
    row_lane = lane[:1]
    docs = doc_ref[...].astype(F32)
    for h in range(pay_ref.shape[0]):
        at = slice(h // 2 * 128, h // 2 * 128 + 128)
        k = keys_ref[:, at].astype(F32)
        v = values_ref[:, at].astype(F32)
        q = queries_ref[:, at].astype(F32)
        q0, q1 = q[: BLK // 2], q[BLK // 2 :]
        if h % 2:
            k, q0 = pltpu.roll(k, 64, 1), pltpu.roll(q0, 64, 1)
        else:
            v, q1 = pltpu.roll(v, 64, 1), pltpu.roll(q1, 64, 1)
        pay_ref[h, 0:BLK, :] = jnp.where(lane < 64, k, v).astype(BF16)
        pay_ref[h, BLK + EXTRA :, :] = jnp.where(half < 64, q0, q1).astype(BF16)
        gate = gate_ref[h : h + 1, :]
        base = gate[:, 0:1]
        rows = [
            p[:, c * 128 : (c + 1) * 128]
            for p in pieces_of((base - gate) * LOG2E)
            for c in range(4)
        ]
        rows += [docs[:, c * 128 : (c + 1) * 128] for c in range(4)]
        b0, b1, b2 = pieces_of(jnp.broadcast_to(base, (1, 128)))
        rows.append(
            jnp.where(
                row_lane == 0,
                b0,
                jnp.where(row_lane == 1, b1, jnp.where(row_lane == 2, b2, 0.0)),
            )
        )
        rows.append(jnp.zeros((15, 128), F32))
        pay_ref[h, BLK : BLK + EXTRA, :] = jnp.concatenate(rows, axis=0).astype(BF16)


def attention_kernel(
    q_hbm, kvx_hbm, gain_ref, o_ref, q_ref, kvx_ref, kp, vt, qp, score_ref, acc, mrow, g0, q_sem, kv_sem
):
    members = kvx_ref.shape[0]
    groups = kvx_ref.shape[1]
    blocks = members * groups
    me = lax.rem(lax.axis_index("sp"), members)
    z = lax.axis_index("sp") // members
    lane = lax.broadcasted_iota(jnp.int32, (128, 128), 1)
    lane_wide = lax.broadcasted_iota(jnp.int32, (BLK, 128), 1)
    row_extra = lax.broadcasted_iota(jnp.int32, (EXTRA, 128), 0)
    is_doc = (row_extra >= 12) & (row_extra < 16)

    def fetch(kb):
        member, group = lax.rem(kb, members), kb // members
        return pltpu.make_async_copy(
            kvx_hbm.at[member, group], kvx_ref.at[member, group], kv_sem.at[kb]
        )

    @pl.loop(0, blocks)
    def _(kb):
        fetch(kb).start()

    q_copy = pltpu.make_async_copy(q_hbm, q_ref, q_sem)
    q_copy.start()

    def prepare(kb, counts):
        member, group = lax.rem(kb, members), kb // members
        fetch(kb).wait()
        extra = kvx_ref[member, group, BLK : BLK + EXTRA, :].astype(F32)
        g0[kb] = jnp.sum(jnp.where(row_extra == 16, extra, 0.0))
        counts = tuple(
            count + jnp.where(is_doc & (extra < d + 0.5), 1.0, 0.0)
            for d, count in enumerate(counts)
        )
        turned = jnp.concatenate([extra, jnp.zeros((128 - EXTRA, 128), F32)], axis=0).T
        for c in range(4):
            kp[kb, c * 128 : (c + 1) * 128, 128:256] = jnp.where(
                (lane < 12) & (lane % 4 == c), turned, 0.0
            ).astype(BF16)
        kv = kvx_ref[member, group, 0:BLK, :].astype(F32)
        kp[kb, :, 0:128] = jnp.where(lane_wide < 64, kv, pltpu.roll(kv, 64, 1)).astype(BF16)
        vt[kb, 16:80, :] = kv.T[64:128, :].astype(BF16)
        vt[kb, 0:16, :] = jnp.ones((16, BLK), BF16)
        return counts

    zero = jnp.zeros((EXTRA, 128), F32)
    counts = lax.fori_loop(0, blocks, prepare, (zero, zero, zero))
    q_copy.wait()
    gains = jnp.broadcast_to(gain_ref[pl.ds(z // 2, 1), :], (128, 128)).T
    gain_column = jnp.where(lax.rem(z, 2) == 0, gains[0:64], gains[64:128])
    starts = [jnp.sum(c).astype(jnp.int32) for c in counts]

    def one_query_block(i, unused):
        qb = i * members + me
        half = q_ref[i].astype(F32) * (LOG2E * 0.125)
        q = jnp.concatenate([half, pltpu.roll(half, 64, 1)], axis=0)
        hi = q.astype(BF16).astype(F32)
        low = pltpu.roll(q - hi, 64, 1)
        qp[:, 0:128] = jnp.where(lane_wide < 64, hi, low).astype(BF16)
        qp[:, 128:256] = jnp.where(lane_wide < 12, 1.0, 0.0).astype(BF16)
        extra = kvx_ref[me, i, BLK : BLK + EXTRA, :].astype(F32)
        doc = jnp.concatenate([extra[12 + c : 13 + c, :] for c in range(4)], axis=1)
        start = jnp.where(
            doc < 0.5,
            0,
            jnp.where(doc < 1.5, starts[0], jnp.where(doc < 2.5, starts[1], starts[2])),
        )
        first = jnp.min(start)
        last = jnp.max(start)
        base = g0[qb]

        first_block = first // BLK
        count = qb - first_block + 1

        def block_at(n):
            return jnp.where(n == 0, qb, jnp.minimum(first_block + n - 1, qb))

        def score_of(kb):
            return lax.dot_general(
                kp[kb], qp[...], (((1,), (1,)), ((), ())), preferred_element_type=F32
            )

        def visit(slot, n, masked):
            kb = block_at(n)
            shift = (base - g0[kb]) * LOG2E
            scores = score_ref[slot]
            if masked:
                key_pos = kb * BLK + lax.broadcasted_iota(jnp.int32, (BLK, BLK), 0)
                query_pos = qb * BLK + lax.broadcasted_iota(jnp.int32, (BLK, BLK), 1)
                allowed = (key_pos <= query_pos) & (key_pos >= start)
                scores = jnp.where(allowed, scores, NEG)
            old = mrow[...]
            top = jnp.maximum(old, jnp.max(scores, axis=0, keepdims=True) + shift)
            score_ref[1 - slot] = score_of(block_at(n + 1))
            weights = jnp.exp2(scores - (top - shift)).astype(BF16)
            added = jnp.dot(vt[kb], weights, preferred_element_type=F32)
            acc[...] = acc[...] * jnp.exp2(old - top) + added
            mrow[...] = top

        mrow[...] = jnp.full((1, BLK), NEG, F32)
        acc[...] = jnp.zeros((80, BLK), F32)
        score_ref[0] = score_of(qb)

        def two_blocks(m, carry):
            for slot in range(2):
                n = 2 * m + slot
                plain = (n > 0) & (block_at(n) * BLK >= last)

                @pl.when((n < count) & plain)
                def _():
                    visit(slot, n, False)

                @pl.when((n < count) & jnp.logical_not(plain))
                def _():
                    visit(slot, n, True)

            return carry

        lax.fori_loop(0, (count + 1) // 2, two_blocks, 0)
        out = acc[16:80, :] / acc[0:1, :]
        mean_square = jnp.mean(out * out, axis=0, keepdims=True)
        gain = jnp.concatenate([gain_column] * 4, axis=1)
        normed = (out * lax.rsqrt(mean_square + EPS) * gain).astype(BF16)
        for c in range(4):
            o_ref[i, c] = normed[:, c * 128 : (c + 1) * 128]
        return unused

    lax.fori_loop(0, groups, one_query_block, 0)


def attend(q, kvx, gain):
    members, groups = kvx.shape[:2]
    blocks = members * groups
    vmem = pl.BlockSpec(memory_space=pltpu.VMEM)
    hbm = pl.BlockSpec(memory_space=pl.ANY)
    return pl.pallas_call(
        attention_kernel,
        out_shape=jax.ShapeDtypeStruct((groups, 4, 64, 128), BF16),
        in_specs=[hbm, hbm, vmem],
        out_specs=vmem,
        scratch_shapes=[
            pltpu.VMEM(q.shape, BF16),
            pltpu.VMEM(kvx.shape, BF16),
            pltpu.VMEM((blocks, BLK, 256), BF16),
            pltpu.VMEM((blocks, 80, BLK), BF16),
            pltpu.VMEM((BLK, 256), BF16),
            pltpu.VMEM((2, BLK, BLK), F32),
            pltpu.VMEM((80, BLK), F32),
            pltpu.VMEM((1, BLK), F32),
            pltpu.SMEM((blocks,), F32),
            pltpu.SemaphoreType.DMA,
            pltpu.SemaphoreType.DMA((blocks,)),
        ],
        compiler_params=pltpu.CompilerParams(vmem_limit_bytes=48 * 1024 * 1024),
        name="attention",
    )(q, kvx, gain)


MESH = pl.DeviceIdType.MESH
GROUP = 2
KVX = BLK + EXTRA


def remote(src, dst, send_sem, recv_sem, sp, tp):
    return pltpu.make_async_remote_copy(
        src_ref=src,
        dst_ref=dst,
        send_sem=send_sem,
        recv_sem=recv_sem,
        device_id=(sp, tp),
        device_id_type=MESH,
    )


def gather_kernel(
    queries_hbm, keys_hbm, values_hbm, gate_hbm, doc_hbm, q_ref, kvx_ref,
    queries_ref, keys_ref, values_ref, gate_ref, doc_ref, in_sem, pay_ref, q_send, q_recv, a_send, a_recv, y_send, y_recv,
    h_send, h_recv, d_send, d_recv,
):
    members, groups = kvx_ref.shape[:2]
    ring = members // 2
    loads = [
        pltpu.make_async_copy(a, b, in_sem.at[i])
        for i, (a, b) in enumerate(
            (
                (queries_hbm, queries_ref),
                (keys_hbm, keys_ref),
                (values_hbm, values_ref),
                (gate_hbm, gate_ref),
                (doc_hbm, doc_ref),
            )
        )
    ]
    for load in loads:
        load.start()
    s = lax.axis_index("sp")
    t = lax.axis_index("tp")
    z, j = s // members, lax.rem(s, members)
    y, core = j // 2, lax.rem(j, 2)

    def member(dy, other=0):
        c = 1 - core if other else core
        return lax.rem(y + dy + ring, ring) * 2 + c

    sides = (member(1), member(-1))
    far = member(2)
    peers = [lax.rem(z + d, groups) * members + j for d in range(1, groups)]
    peers += [z * members + m for m in (*sides, member(0, 1))]
    barrier = pltpu.get_barrier_semaphore()
    for peer in peers:
        pl.semaphore_signal(barrier, 1, device_id=(peer, t), device_id_type=MESH)
    for load in loads:
        load.wait()
    pack(queries_ref, keys_ref, values_ref, gate_ref, doc_ref, pay_ref)
    pl.semaphore_wait(barrier, len(peers))

    order = (0, 1, 3, 2)

    def kv_copy(n, d, source):
        to = lax.rem(z + d, groups)
        return remote(
            pay_ref.at[to, pl.ds(0, KVX)], kvx_ref.at[j, source], a_send, a_recv.at[n],
            to * members + j, t,
        )

    def q_copy(n, d, source):
        to = lax.rem(z + d, groups)
        return remote(
            pay_ref.at[to, pl.ds(KVX, BLK // 2)], q_ref.at[source], q_send, q_recv.at[n],
            to * members + j, t,
        )

    for n, d in enumerate(order):
        if d:
            kv_copy(n, d, z).start()
    for n, d in enumerate(order):
        if d:
            q_copy(n, d, z).start()
    kvx_ref[j, z] = pay_ref[z, 0:KVX, :]
    q_ref[z] = pay_ref[z, KVX : KVX + BLK // 2, :]

    def source_of(n):
        return lax.rem(z - order[n] + groups, groups)

    def to_side(i, rows, send_sem, recv_sem):
        return remote(rows, rows, send_sem, recv_sem, z * members + sides[i], t)

    def to_core(kind, n, m):
        rows = kvx_ref.at[m, source_of(n)]
        return remote(
            rows, rows, d_send, d_recv.at[kind, n], z * members + member(0, 1), t
        )

    def piece(i):
        return pl.ds(i * (KVX // 2), KVX // 2)

    def enter(n):
        if n:
            kv_copy(n, order[n], source_of(n)).wait_recv()
        rows = kvx_ref.at[j, source_of(n)]
        for i in range(2):
            to_side(i, rows, y_send.at[i], y_recv.at[i, n]).start()
        to_core(0, n, j).start()

    def relay(n):
        for i in range(2):
            origin = sides[1 - i]
            rows = kvx_ref.at[origin, source_of(n)]
            to_side(i, rows, y_send.at[i], y_recv.at[i, n]).wait_recv()
            rows = kvx_ref.at[origin, source_of(n), piece(i)]
            to_side(i, rows, h_send.at[i], h_recv.at[i, n]).start()
            to_core(1 + i, n, origin).start()

    def finish(n):
        for i in range(2):
            rows = kvx_ref.at[far, source_of(n), piece(i)]
            to_side(i, rows, h_send.at[i], h_recv.at[i, n]).wait_recv()
        to_core(3, n, far).start()

    for step in range(groups + 2):
        if step < groups:
            enter(step)
        if 1 <= step <= groups:
            relay(step - 1)
        if step >= 2:
            finish(step - 2)
    for n in range(groups):
        for kind in range(4):
            to_core(kind, n, member((0, -1, 1, 2)[kind], 1)).wait_recv()
    for n in range(1, groups):
        q_copy(n, order[n], source_of(n)).wait_recv()
    for n in range(1, groups):
        kv_copy(n, order[n], z).wait_send()
        q_copy(n, order[n], z).wait_send()
    rows = kvx_ref.at[j]
    halves = kvx_ref.at[0, :, pl.ds(0, KVX // 2)]
    for i in range(2):
        to_side(i, rows, y_send.at[i], y_recv.at[i, 0]).wait_send()
        to_side(i, halves, h_send.at[i], h_recv.at[i, 0]).wait_send()
    every = kvx_ref.at[pl.ds(0, 4)]
    remote(every, every, d_send, d_recv.at[0, 0], z * members, t).wait_send()


def gather_history(queries, keys, values, gate, documents, members):
    groups = gate.shape[0]
    vmem = pl.BlockSpec(memory_space=pltpu.VMEM)
    dma = pltpu.SemaphoreType.DMA
    return pl.pallas_call(
        gather_kernel,
        out_shape=(
            jax.ShapeDtypeStruct((groups, BLK // 2, 128), BF16),
            jax.ShapeDtypeStruct((members, groups, KVX, 128), BF16),
        ),
        in_specs=[pl.BlockSpec(memory_space=pl.ANY)] * 5,
        out_specs=(vmem, vmem),
        scratch_shapes=[
            *(pltpu.VMEM(a.shape, a.dtype) for a in (queries, keys, values, gate, documents)),
            dma((5,)),
            pltpu.VMEM((groups, KVX + BLK // 2, 128), BF16),
            dma,
            dma((groups,)),
            dma,
            dma((groups,)),
            dma((2,)),
            dma((2, groups)),
            dma((2,)),
            dma((2, groups)),
            dma,
            dma((4, groups)),
        ],
        compiler_params=pltpu.CompilerParams(
            collective_id=0, has_side_effects=True, vmem_limit_bytes=16 * 1024 * 1024
        ),
        name="gather_history",
    )(queries, keys, values, gate, documents)


def experts_kernel(
    normed_ref, ow_hbm, resid_hbm, ng_ref, routes_ref, rw_ref, wg_hbm, wu_hbm, wd_hbm,
    mixed_ref,
    heads, ow, resid_ref, stream, spread_ref, out_ref, ret_ref, x, p, r_in, m_in, wg, wu, wd,
    w_sem, head_send, head_recv, a2a_send, a2a_recv, ag_send, ag_recv, relay_send, relay_recv,
    r_send, r_recv, m_send, m_recv, ret_send, ret_recv,
):
    experts, slots, width = out_ref.shape
    groups = normed_ref.shape[0]
    tps = x.shape[0]
    members = experts // groups
    steps = experts // GROUP
    half = GROUP // 2
    send = remote
    s = lax.axis_index("sp")
    t = lax.axis_index("tp")
    z, j = s // members, lax.rem(s, members)
    right = lax.rem(t + 1, tps)
    left = lax.rem(t + tps - 1, tps)
    far = lax.rem(t + 2, tps)
    sides = (right, left)

    loads = [
        pltpu.make_async_copy(a, b, w_sem.at[i])
        for i, (a, b) in enumerate(
            ((ow_hbm, ow), (resid_hbm, resid_ref), (wg_hbm.at[0], wg), (wu_hbm.at[0], wu), (wd_hbm.at[0], wd))
        )
    ]
    for load in loads:
        load.start()

    barrier = pltpu.get_barrier_semaphore()

    @pl.loop(1, experts)
    def _(k):
        pl.semaphore_signal(
            barrier, 1, device_id=(lax.rem(s + k, experts), t), device_id_type=MESH
        )

    for side in sides:
        pl.semaphore_signal(barrier, 1, device_id=(s, side), device_id_type=MESH)

    def owner(n):
        return lax.rem(z + n // tps, groups), lax.rem(t + lax.rem(n, tps), tps)

    @pl.loop(1, groups * tps)
    def _(n):
        zz, tt = owner(n)
        pl.semaphore_signal(barrier, 1, device_id=(zz * members + j, tt), device_id_type=MESH)

    pl.semaphore_wait(barrier, experts - 1 + 2 + groups * tps - 1)

    mine = t * groups + z

    @pl.loop(1, groups * tps)
    def _(n):
        zz, tt = owner(n)
        send(
            normed_ref.at[zz, tt], heads.at[mine], head_send, head_recv, zz * members + j, tt
        ).start()

    heads[mine] = normed_ref[z, t]
    rows = normed_ref.shape[3]
    picked = jnp.concatenate(
        [routes_ref[...].astype(F32), rw_ref[...], jnp.zeros((rows - 4, rows), F32)], axis=0
    ).T
    lane = lax.broadcasted_iota(jnp.int32, (rows, rows), 1)
    below = lane < lax.broadcasted_iota(jnp.int32, (rows, rows), 0)
    named = [jnp.where(lane.astype(F32) == picked[:, k : k + 1], 1.0, 0.0) for k in range(2)]
    earlier = jnp.dot(
        jnp.where(below, 1.0, 0.0).astype(BF16),
        (named[0] + named[1]).astype(BF16),
        preferred_element_type=F32,
    )
    slot_lane = lax.broadcasted_iota(jnp.int32, (rows, experts * slots), 1).astype(F32)
    taken = [
        slot_lane
        == picked[:, k : k + 1] * slots + jnp.sum(named[k] * earlier, axis=1, keepdims=True)
        for k in range(2)
    ]
    chosen = jnp.where(taken[0] | taken[1], 1.0, 0.0).astype(BF16)
    spread_ref[...] = jnp.where(taken[0], picked[:, 2:3], 0.0) + jnp.where(
        taken[1], picked[:, 3:4], 0.0
    )
    loads[0].wait()
    loads[1].wait()
    others = heads.at[pl.ds(0, groups * tps - 1)]
    send(others, others, head_send, head_recv, s, right).wait()
    projected = lax.dot_general(
        heads[...].reshape(groups * tps * 64, 128), ow[...], (((0,), (0,)), ((), ())),
        preferred_element_type=F32,
    )
    stream[...] = (resid_ref[...].astype(F32) + projected).astype(BF16)
    widened = stream[...].astype(F32)
    mean_wide = jnp.mean(widened * widened, axis=-1, keepdims=True)
    expert_input = (widened * lax.rsqrt(mean_wide + EPS) * ng_ref[...]).astype(BF16)
    out_ref[...] = (
        lax.dot_general(
            chosen, expert_input, (((0,), (0,)), ((), ())), preferred_element_type=F32
        )
        .astype(BF16)
        .reshape(experts, slots, width)
    )

    def to_side(i, src, dst, send_sem, recv_sem):
        return send(src, dst, send_sem, recv_sem, s, sides[i])

    @pl.loop(1, experts)
    def _(k):
        to = lax.rem(s + k, experts)
        send(out_ref.at[to], x.at[t, k], a2a_send, a2a_recv.at[k // GROUP], to, t).start()

    x[t, 0] = out_ref[s]

    def whole(c):
        return pl.ds(c * GROUP, GROUP)

    def part(c, i):
        return pl.ds(c * GROUP + i * half, half)

    def enter(c):
        @pl.when(c == 0)
        def _():
            first = x.at[t, pl.ds(1, GROUP - 1)]
            send(first, first, a2a_send, a2a_recv.at[0], s, right).wait_recv()

        @pl.when(c > 0)
        def _():
            rows = x.at[t, whole(c)]
            send(rows, rows, a2a_send, a2a_recv.at[c], s, right).wait_recv()

        rows = x.at[t, whole(c)]
        for i in range(2):
            to_side(i, rows, rows, ag_send.at[i], ag_recv.at[i, c]).start()

    def relay(c):
        for i in range(2):
            origin = sides[1 - i]
            rows = x.at[origin, whole(c)]
            to_side(i, rows, rows, ag_send.at[i], ag_recv.at[i, c]).wait_recv()
            rows = x.at[origin, part(c, i)]
            to_side(i, rows, rows, relay_send.at[i], relay_recv.at[i, c]).start()

    def compute(c):
        for i in range(2):
            rows = x.at[far, part(c, i)]
            to_side(i, rows, rows, relay_send.at[i], relay_recv.at[i, c]).wait_recv()
        rows = x[:, whole(c)].reshape(tps * GROUP * slots, width)
        gate = jnp.dot(rows, wg[...], preferred_element_type=F32)
        up = jnp.dot(rows, wu[...], preferred_element_type=F32)
        hidden = (gate / (1.0 + jnp.exp(-gate)) * up).astype(BF16)
        made = jnp.dot(hidden, wd[...], preferred_element_type=F32)
        p[:, whole(c)] = made.astype(BF16).reshape(tps, GROUP, slots, width)
        for i in range(2):
            to_side(
                i, p.at[far, part(c, i)], r_in.at[i, pl.ds(c * half, half)],
                r_send.at[i], r_recv.at[i, c],
            ).start()

    def pass_on(c):
        for i in range(2):
            got = r_in.at[i, pl.ds(c * half, half)]
            to_side(i, got, got, r_send.at[i], r_recv.at[i, c]).wait_recv()
            mine = p[sides[i], part(c, i)].astype(F32)
            p[sides[i], part(c, i)] = (mine + got[...].astype(F32)).astype(BF16)
        for i in range(2):
            to_side(
                i, p.at[sides[i], whole(c)], m_in.at[i, whole(c)], m_send.at[i], m_recv.at[i, c]
            ).start()

    def leave(c):
        total = p[t, whole(c)].astype(F32)
        for i in range(2):
            got = m_in.at[i, whole(c)]
            to_side(i, got, got, m_send.at[i], m_recv.at[i, c]).wait_recv()
            total = total + got[...].astype(F32)
        p[t, whole(c)] = total.astype(BF16)

        @pl.when(c == 0)
        def _():
            ret_ref[s] = p[t, 0]

        @pl.loop(jnp.where(c == 0, 1, 0), GROUP)
        def _(j):
            k = c * GROUP + j
            to = lax.rem(s + experts - k, experts)
            send(p.at[t, k], ret_ref.at[s], ret_send, ret_recv, to, t).start()

    @pl.loop(0, steps + 4)
    def _(i):
        @pl.when(i < steps)
        def _():
            enter(i)

        @pl.when((i >= 1) & (i < steps + 1))
        def _():
            relay(i - 1)

        @pl.when(i >= 4)
        def _():
            leave(i - 4)

        @pl.when((i >= 3) & (i < steps + 3))
        def _():
            pass_on(i - 3)

        @pl.when(i == 2)
        def _():
            for load in loads[2:]:
                load.wait()

        @pl.when((i >= 2) & (i < steps + 2))
        def _():
            compute(i - 2)

    most = x.at[0, pl.ds(0, experts - 1)]
    every = x.at[0]
    some = x.at[0, pl.ds(0, experts // 2)]
    back = ret_ref.at[pl.ds(0, experts - 1)]
    send(most, back, a2a_send, ret_recv, s, right).wait_send()
    send(most, back, ret_send, ret_recv, s, right).wait()
    for i in range(2):
        to_side(i, every, every, ag_send.at[i], ag_recv.at[i, 0]).wait_send()
        to_side(i, some, some, relay_send.at[i], relay_recv.at[i, 0]).wait_send()
        to_side(i, some, some, r_send.at[i], r_recv.at[i, 0]).wait_send()
        to_side(i, every, every, m_send.at[i], m_recv.at[i, 0]).wait_send()
    spread = spread_ref[...]
    results = ret_ref[...].reshape(experts * slots, width)
    mixed = stream[...].astype(F32)
    for _ in range(3):
        digit = spread.astype(BF16)
        mixed = mixed + jnp.dot(digit, results, preferred_element_type=F32)
        spread = spread - digit.astype(F32)
    mixed_ref[...] = mixed.astype(BF16)


def at_experts(normed, out_weight, resid, norm_gain, routes, route_weights, w_gate, w_up, w_down):
    groups, tps = normed.shape[:2]
    rows, width = resid.shape
    hidden = w_gate.shape[2]
    experts = lax.axis_size("sp")
    slots = 16
    steps = experts // GROUP
    vmem = pl.BlockSpec(memory_space=pltpu.VMEM)
    hbm = pl.BlockSpec(memory_space=pl.ANY)
    dma = pltpu.SemaphoreType.DMA
    return pl.pallas_call(
        experts_kernel,
        out_shape=jax.ShapeDtypeStruct((rows, width), BF16),
        in_specs=[vmem, hbm, hbm, vmem, vmem, vmem, hbm, hbm, hbm],
        out_specs=vmem,
        scratch_shapes=[
            pltpu.VMEM((groups * tps, 64, 128), BF16),
            pltpu.VMEM(out_weight.shape, BF16),
            pltpu.VMEM((rows, width), BF16),
            pltpu.VMEM((rows, width), BF16),
            pltpu.VMEM((rows, experts * slots), F32),
            pltpu.VMEM((experts, slots, width), BF16),
            pltpu.VMEM((experts, slots, width), BF16),
            pltpu.VMEM((tps, experts, slots, width), BF16),
            pltpu.VMEM((tps, experts, slots, width), BF16),
            pltpu.VMEM((2, experts // 2, slots, width), BF16),
            pltpu.VMEM((2, experts, slots, width), BF16),
            pltpu.VMEM((width, hidden), BF16),
            pltpu.VMEM((width, hidden), BF16),
            pltpu.VMEM((hidden, width), BF16),
            dma((5,)),
            dma,
            dma,
            dma,
            dma((steps,)),
            dma((2,)),
            dma((2, steps)),
            dma((2,)),
            dma((2, steps)),
            dma((2,)),
            dma((2, steps)),
            dma((2,)),
            dma((2, steps)),
            dma,
            dma,
        ],
        compiler_params=pltpu.CompilerParams(
            collective_id=1, has_side_effects=True, vmem_limit_bytes=60 * 1024 * 1024
        ),
        name="experts",
    )(
        normed, out_weight, resid, norm_gain.reshape(1, width), routes.T, route_weights.T,
        w_gate, w_up, w_down,
    )


def on_device(
    queries,
    keys,
    values,
    cum_gate,
    documents,
    head_gain,
    out_weight,
    resid,
    norm_gain,
    routes,
    route_weights,
    w_gate,
    w_up,
    w_down,
):
    tokens = queries.shape[0]
    heads = cum_gate.shape[1]
    sp_count = lax.axis_size("sp")
    members = sp_count // heads
    q, kvx = gather_history(
        queries, keys, values, cum_gate.T, documents.reshape(1, tokens), members
    )
    gain = head_gain.reshape(2, 128)
    normed = attend(q, kvx, gain)
    return at_experts(
        normed, out_weight, resid, norm_gain, routes, route_weights, w_gate, w_up, w_down
    )


def solution(mesh):
    in_specs = (
        P("sp", "tp"),
        P("sp", "tp"),
        P("sp", "tp"),
        P("sp", "tp"),
        P("sp"),
        P("tp"),
        P(),
        P(("sp", "tp"), None),
        P(),
        P(("sp", "tp"), None),
        P(("sp", "tp"), None),
        P("sp", None, "tp"),
        P("sp", None, "tp"),
        P("sp", "tp", None),
    )
    out_specs = P(("sp", "tp"), None)
    return jax.shard_map(
        on_device, mesh=mesh, in_specs=in_specs, out_specs=out_specs, check_vma=False
    )
```

```python
import jax
import jax.numpy as jnp
from jax import lax
from jax.experimental import pallas as pl
from jax.experimental.pallas import tpu as pltpu
from jax.sharding import PartitionSpec as P

EPS = 1e-06
LOG2E = 1.4426950408889634
BLK = 512
EXTRA = 32
NEG = -1e30
F32 = jnp.float32
BF16 = jnp.bfloat16


def pieces_of(x):
    hi = x.astype(BF16).astype(F32)
    rest = x - hi
    mid = rest.astype(BF16).astype(F32)
    return hi, mid, rest - mid


def pack(qkv_ref, small_ref, pay_ref):
    lane = lax.broadcasted_iota(jnp.int32, (BLK, 128), 1)
    half = lane[: BLK // 2]
    row_lane = lane[:1]
    heads = pay_ref.shape[0]
    docs = small_ref[heads : heads + 1, :]
    for h in range(heads):
        at = slice(h // 2 * 128, h // 2 * 128 + 128)
        q = qkv_ref[0:BLK, at].astype(F32)
        k = qkv_ref[BLK : 2 * BLK, at].astype(F32)
        v = qkv_ref[2 * BLK : 3 * BLK, at].astype(F32)
        q0, q1 = q[: BLK // 2], q[BLK // 2 :]
        if h % 2:
            k, q0 = pltpu.roll(k, 64, 1), pltpu.roll(q0, 64, 1)
        else:
            v, q1 = pltpu.roll(v, 64, 1), pltpu.roll(q1, 64, 1)
        pay_ref[h, 0:BLK, :] = jnp.where(lane < 64, k, v).astype(BF16)
        pay_ref[h, BLK + EXTRA :, :] = jnp.where(half < 64, q0, q1).astype(BF16)
        gate = small_ref[h : h + 1, :]
        base = gate[:, 0:1]
        rows = [
            p[:, c * 128 : (c + 1) * 128]
            for p in pieces_of((base - gate) * LOG2E)
            for c in range(4)
        ]
        rows += [docs[:, c * 128 : (c + 1) * 128] for c in range(4)]
        b0, b1, b2 = pieces_of(jnp.broadcast_to(base, (1, 128)))
        rows.append(
            jnp.where(
                row_lane == 0,
                b0,
                jnp.where(row_lane == 1, b1, jnp.where(row_lane == 2, b2, 0.0)),
            )
        )
        rows.append(jnp.zeros((15, 128), F32))
        pay_ref[h, BLK : BLK + EXTRA, :] = jnp.concatenate(rows, axis=0).astype(BF16)


def attention_kernel(
    q_ref, kvx_ref, small_ref, o_ref, kp, vt, qp, score_ref, acc, mrow, g0
):
    members = kvx_ref.shape[0]
    groups = kvx_ref.shape[1]
    blocks = members * groups
    me = lax.rem(lax.axis_index("sp"), members)
    z = lax.axis_index("sp") // members
    lane = lax.broadcasted_iota(jnp.int32, (128, 128), 1)
    lane_wide = lax.broadcasted_iota(jnp.int32, (BLK, 128), 1)
    row_extra = lax.broadcasted_iota(jnp.int32, (EXTRA, 128), 0)
    is_doc = (row_extra >= 12) & (row_extra < 16)

    def prepare(kb, counts):
        member, group = lax.rem(kb, members), kb // members
        extra = kvx_ref[member, group, BLK : BLK + EXTRA, :].astype(F32)
        g0[kb] = jnp.sum(jnp.where(row_extra == 16, extra, 0.0))
        counts = tuple(
            count + jnp.where(is_doc & (extra < d + 0.5), 1.0, 0.0)
            for d, count in enumerate(counts)
        )
        turned = jnp.concatenate([extra, jnp.zeros((128 - EXTRA, 128), F32)], axis=0).T
        for c in range(4):
            kp[kb, c * 128 : (c + 1) * 128, 128:256] = jnp.where(
                (lane < 12) & (lane % 4 == c), turned, 0.0
            ).astype(BF16)
        kv = kvx_ref[member, group, 0:BLK, :].astype(F32)
        kp[kb, :, 0:128] = jnp.where(lane_wide < 64, kv, pltpu.roll(kv, 64, 1)).astype(BF16)
        vt[kb, 16:80, :] = kv.T[64:128, :].astype(BF16)
        vt[kb, 0:16, :] = jnp.ones((16, BLK), BF16)
        return counts

    zero = jnp.zeros((EXTRA, 128), F32)
    counts = lax.fori_loop(0, blocks, prepare, (zero, zero, zero))
    gain_row = jnp.where(z < 2, small_ref[5:6, 0:128], small_ref[5:6, 128:256])
    gains = jnp.broadcast_to(gain_row, (128, 128)).T
    gain_column = jnp.where(lax.rem(z, 2) == 0, gains[0:64], gains[64:128])
    starts = [jnp.sum(c).astype(jnp.int32) for c in counts]

    def one_query_block(i, unused):
        qb = i * members + me
        half = q_ref[i].astype(F32) * (LOG2E * 0.125)
        q = jnp.concatenate([half, pltpu.roll(half, 64, 1)], axis=0)
        hi = q.astype(BF16).astype(F32)
        low = pltpu.roll(q - hi, 64, 1)
        qp[:, 0:128] = jnp.where(lane_wide < 64, hi, low).astype(BF16)
        qp[:, 128:256] = jnp.where(lane_wide < 12, 1.0, 0.0).astype(BF16)
        extra = kvx_ref[me, i, BLK : BLK + EXTRA, :].astype(F32)
        doc = jnp.concatenate([extra[12 + c : 13 + c, :] for c in range(4)], axis=1)
        start = jnp.where(
            doc < 0.5,
            0,
            jnp.where(doc < 1.5, starts[0], jnp.where(doc < 2.5, starts[1], starts[2])),
        )
        first = jnp.min(start)
        last = jnp.max(start)
        base = g0[qb]

        first_block = first // BLK
        count = qb - first_block + 1

        def block_at(n):
            return jnp.where(n == 0, qb, jnp.minimum(first_block + n - 1, qb))

        def score_of(kb):
            return lax.dot_general(
                kp[kb], qp[...], (((1,), (1,)), ((), ())), preferred_element_type=F32
            )

        def visit(slot, n, masked):
            kb = block_at(n)
            shift = (base - g0[kb]) * LOG2E
            scores = score_ref[slot]
            if masked:
                key_pos = kb * BLK + lax.broadcasted_iota(jnp.int32, (BLK, BLK), 0)
                query_pos = qb * BLK + lax.broadcasted_iota(jnp.int32, (BLK, BLK), 1)
                allowed = (key_pos <= query_pos) & (key_pos >= start)
                scores = jnp.where(allowed, scores, NEG)
            old = mrow[...]
            top = jnp.maximum(old, jnp.max(scores, axis=0, keepdims=True) + shift)
            score_ref[1 - slot] = score_of(block_at(n + 1))
            weights = jnp.exp2(scores - (top - shift)).astype(BF16)
            added = jnp.dot(vt[kb], weights, preferred_element_type=F32)
            acc[...] = acc[...] * jnp.exp2(old - top) + added
            mrow[...] = top

        mrow[...] = jnp.full((1, BLK), NEG, F32)
        acc[...] = jnp.zeros((80, BLK), F32)
        score_ref[0] = score_of(qb)

        def two_blocks(m, carry):
            for slot in range(2):
                n = 2 * m + slot
                plain = (n > 0) & (block_at(n) * BLK >= last)

                @pl.when((n < count) & plain)
                def _():
                    visit(slot, n, False)

                @pl.when((n < count) & jnp.logical_not(plain))
                def _():
                    visit(slot, n, True)

            return carry

        lax.fori_loop(0, (count + 1) // 2, two_blocks, 0)
        out = acc[16:80, :] / acc[0:1, :]
        mean_square = jnp.mean(out * out, axis=0, keepdims=True)
        gain = jnp.concatenate([gain_column] * 4, axis=1)
        normed = (out * lax.rsqrt(mean_square + EPS) * gain).astype(BF16)
        for c in range(4):
            o_ref[i, c] = normed[:, c * 128 : (c + 1) * 128]
        return unused

    lax.fori_loop(0, groups, one_query_block, 0)


def attend(q, kvx, small):
    members, groups = kvx.shape[:2]
    blocks = members * groups
    vmem = pl.BlockSpec(memory_space=pltpu.VMEM)
    hbm = pl.BlockSpec(memory_space=pltpu.HBM)
    return pl.pallas_call(
        attention_kernel,
        out_shape=jax.ShapeDtypeStruct((groups, 4, 64, 128), BF16),
        in_specs=[vmem, vmem, vmem],
        out_specs=vmem,
        scratch_shapes=[
            pltpu.VMEM((blocks, BLK, 256), BF16),
            pltpu.VMEM((blocks, 80, BLK), BF16),
            pltpu.VMEM((BLK, 256), BF16),
            pltpu.VMEM((2, BLK, BLK), F32),
            pltpu.VMEM((80, BLK), F32),
            pltpu.VMEM((1, BLK), F32),
            pltpu.SMEM((blocks,), F32),
        ],
        compiler_params=pltpu.CompilerParams(vmem_limit_bytes=48 * 1024 * 1024),
        name="attention",
    )(q, kvx, small)


MESH = pl.DeviceIdType.MESH
GROUP = 2
KVX = BLK + EXTRA


def remote(src, dst, send_sem, recv_sem, sp, tp):
    return pltpu.make_async_remote_copy(
        src_ref=src,
        dst_ref=dst,
        send_sem=send_sem,
        recv_sem=recv_sem,
        device_id=(sp, tp),
        device_id_type=MESH,
    )


def gather_kernel(
    qkv_ref, small_ref, q_ref, kvx_ref, pay_ref, q_send, q_recv, a_send, a_recv, y_send, y_recv,
    h_send, h_recv, d_send, d_recv,
):
    members, groups = kvx_ref.shape[:2]
    ring = members // 2
    s = lax.axis_index("sp")
    t = lax.axis_index("tp")
    z, j = s // members, lax.rem(s, members)
    y, core = j // 2, lax.rem(j, 2)

    def member(dy, other=0):
        c = 1 - core if other else core
        return lax.rem(y + dy + ring, ring) * 2 + c

    sides = (member(1), member(-1))
    far = member(2)
    peers = [lax.rem(z + d, groups) * members + j for d in range(1, groups)]
    peers += [z * members + m for m in (*sides, member(0, 1))]
    barrier = pltpu.get_barrier_semaphore()
    for peer in peers:
        pl.semaphore_signal(barrier, 1, device_id=(peer, t), device_id_type=MESH)
    pack(qkv_ref, small_ref, pay_ref)
    pl.semaphore_wait(barrier, len(peers))

    order = (0, 1, 3, 2)

    def kv_copy(n, d, source):
        to = lax.rem(z + d, groups)
        return remote(
            pay_ref.at[to, pl.ds(0, KVX)], kvx_ref.at[j, source], a_send, a_recv.at[n],
            to * members + j, t,
        )

    def q_copy(n, d, source):
        to = lax.rem(z + d, groups)
        return remote(
            pay_ref.at[to, pl.ds(KVX, BLK // 2)], q_ref.at[source], q_send, q_recv.at[n],
            to * members + j, t,
        )

    for n, d in enumerate(order):
        if d:
            kv_copy(n, d, z).start()
    for n, d in enumerate(order):
        if d:
            q_copy(n, d, z).start()
    kvx_ref[j, z] = pay_ref[z, 0:KVX, :]
    q_ref[z] = pay_ref[z, KVX : KVX + BLK // 2, :]

    def source_of(n):
        return lax.rem(z - order[n] + groups, groups)

    def to_side(i, rows, send_sem, recv_sem):
        return remote(rows, rows, send_sem, recv_sem, z * members + sides[i], t)

    def to_core(kind, n, m):
        rows = kvx_ref.at[m, source_of(n)]
        return remote(
            rows, rows, d_send, d_recv.at[kind, n], z * members + member(0, 1), t
        )

    def piece(i):
        return pl.ds(i * (KVX // 2), KVX // 2)

    def enter(n):
        if n:
            kv_copy(n, order[n], source_of(n)).wait_recv()
        rows = kvx_ref.at[j, source_of(n)]
        for i in range(2):
            to_side(i, rows, y_send.at[i], y_recv.at[i, n]).start()
        to_core(0, n, j).start()

    def relay(n):
        for i in range(2):
            origin = sides[1 - i]
            rows = kvx_ref.at[origin, source_of(n)]
            to_side(i, rows, y_send.at[i], y_recv.at[i, n]).wait_recv()
            rows = kvx_ref.at[origin, source_of(n), piece(i)]
            to_side(i, rows, h_send.at[i], h_recv.at[i, n]).start()
            to_core(1 + i, n, origin).start()

    def finish(n):
        for i in range(2):
            rows = kvx_ref.at[far, source_of(n), piece(i)]
            to_side(i, rows, h_send.at[i], h_recv.at[i, n]).wait_recv()
        to_core(3, n, far).start()

    for step in range(groups + 2):
        if step < groups:
            enter(step)
        if 1 <= step <= groups:
            relay(step - 1)
        if step >= 2:
            finish(step - 2)
    for n in range(groups):
        for kind in range(4):
            to_core(kind, n, member((0, -1, 1, 2)[kind], 1)).wait_recv()
    for n in range(1, groups):
        q_copy(n, order[n], source_of(n)).wait_recv()
    for n in range(1, groups):
        kv_copy(n, order[n], z).wait_send()
        q_copy(n, order[n], z).wait_send()
    rows = kvx_ref.at[j]
    halves = kvx_ref.at[0, :, pl.ds(0, KVX // 2)]
    for i in range(2):
        to_side(i, rows, y_send.at[i], y_recv.at[i, 0]).wait_send()
        to_side(i, halves, h_send.at[i], h_recv.at[i, 0]).wait_send()
    every = kvx_ref.at[pl.ds(0, 4)]
    remote(every, every, d_send, d_recv.at[0, 0], z * members, t).wait_send()


def gather_history(qkv, small, groups, members):
    vmem = pl.BlockSpec(memory_space=pltpu.VMEM)
    dma = pltpu.SemaphoreType.DMA
    return pl.pallas_call(
        gather_kernel,
        out_shape=(
            jax.ShapeDtypeStruct((groups, BLK // 2, 128), BF16),
            jax.ShapeDtypeStruct((members, groups, KVX, 128), BF16),
        ),
        in_specs=[vmem] * 2,
        out_specs=(vmem, vmem),
        scratch_shapes=[
            pltpu.VMEM((groups, KVX + BLK // 2, 128), BF16),
            dma,
            dma((groups,)),
            dma,
            dma((groups,)),
            dma((2,)),
            dma((2, groups)),
            dma((2,)),
            dma((2, groups)),
            dma,
            dma((4, groups)),
        ],
        compiler_params=pltpu.CompilerParams(
            collective_id=0, has_side_effects=True, vmem_limit_bytes=16 * 1024 * 1024
        ),
        name="gather_history",
    )(qkv, small)


def experts_kernel(
    normed_ref, ow_hbm, resid_hbm, ng_ref, routes_ref, rw_ref, wg_hbm, wu_hbm, wd_hbm,
    mixed_ref,
    heads, ow, resid_ref, stream, spread_ref, out_ref, ret_ref, x, p, r_in, m_in, wg, wu, wd,
    w_sem, head_send, head_recv, a2a_send, a2a_recv, ag_send, ag_recv, relay_send, relay_recv,
    r_send, r_recv, m_send, m_recv, ret_send, ret_recv,
):
    experts, slots, width = out_ref.shape
    groups = normed_ref.shape[0]
    tps = x.shape[0]
    members = experts // groups
    steps = experts // GROUP
    half = GROUP // 2
    send = remote
    s = lax.axis_index("sp")
    t = lax.axis_index("tp")
    z, j = s // members, lax.rem(s, members)
    right = lax.rem(t + 1, tps)
    left = lax.rem(t + tps - 1, tps)
    far = lax.rem(t + 2, tps)
    sides = (right, left)

    loads = [
        pltpu.make_async_copy(a, b, w_sem.at[i])
        for i, (a, b) in enumerate(
            ((ow_hbm, ow), (resid_hbm, resid_ref), (wg_hbm.at[0], wg), (wu_hbm.at[0], wu), (wd_hbm.at[0], wd))
        )
    ]
    for load in loads:
        load.start()

    barrier = pltpu.get_barrier_semaphore()

    @pl.loop(1, experts)
    def _(k):
        pl.semaphore_signal(
            barrier, 1, device_id=(lax.rem(s + k, experts), t), device_id_type=MESH
        )

    for side in sides:
        pl.semaphore_signal(barrier, 1, device_id=(s, side), device_id_type=MESH)

    def owner(n):
        return lax.rem(z + n // tps, groups), lax.rem(t + lax.rem(n, tps), tps)

    @pl.loop(1, groups * tps)
    def _(n):
        zz, tt = owner(n)
        pl.semaphore_signal(barrier, 1, device_id=(zz * members + j, tt), device_id_type=MESH)

    pl.semaphore_wait(barrier, experts - 1 + 2 + groups * tps - 1)

    mine = t * groups + z

    @pl.loop(1, groups * tps)
    def _(n):
        zz, tt = owner(n)
        send(
            normed_ref.at[zz, tt], heads.at[mine], head_send, head_recv, zz * members + j, tt
        ).start()

    heads[mine] = normed_ref[z, t]
    rows = normed_ref.shape[3]
    picked = jnp.concatenate(
        [routes_ref[...].astype(F32), rw_ref[...], jnp.zeros((rows - 4, rows), F32)], axis=0
    ).T
    lane = lax.broadcasted_iota(jnp.int32, (rows, rows), 1)
    below = lane < lax.broadcasted_iota(jnp.int32, (rows, rows), 0)
    named = [jnp.where(lane.astype(F32) == picked[:, k : k + 1], 1.0, 0.0) for k in range(2)]
    earlier = jnp.dot(
        jnp.where(below, 1.0, 0.0).astype(BF16),
        (named[0] + named[1]).astype(BF16),
        preferred_element_type=F32,
    )
    slot_lane = lax.broadcasted_iota(jnp.int32, (rows, experts * slots), 1).astype(F32)
    taken = [
        slot_lane
        == picked[:, k : k + 1] * slots + jnp.sum(named[k] * earlier, axis=1, keepdims=True)
        for k in range(2)
    ]
    chosen = jnp.where(taken[0] | taken[1], 1.0, 0.0).astype(BF16)
    spread_ref[...] = jnp.where(taken[0], picked[:, 2:3], 0.0) + jnp.where(
        taken[1], picked[:, 3:4], 0.0
    )
    loads[0].wait()
    loads[1].wait()
    others = heads.at[pl.ds(0, groups * tps - 1)]
    send(others, others, head_send, head_recv, s, right).wait()
    projected = lax.dot_general(
        heads[...].reshape(groups * tps * 64, 128), ow[...], (((0,), (0,)), ((), ())),
        preferred_element_type=F32,
    )
    stream[...] = (resid_ref[...].astype(F32) + projected).astype(BF16)
    widened = stream[...].astype(F32)
    mean_wide = jnp.mean(widened * widened, axis=-1, keepdims=True)
    expert_input = (widened * lax.rsqrt(mean_wide + EPS) * ng_ref[...]).astype(BF16)
    out_ref[...] = (
        lax.dot_general(
            chosen, expert_input, (((0,), (0,)), ((), ())), preferred_element_type=F32
        )
        .astype(BF16)
        .reshape(experts, slots, width)
    )

    def to_side(i, src, dst, send_sem, recv_sem):
        return send(src, dst, send_sem, recv_sem, s, sides[i])

    @pl.loop(1, experts)
    def _(k):
        to = lax.rem(s + k, experts)
        send(out_ref.at[to], x.at[t, k], a2a_send, a2a_recv.at[k // GROUP], to, t).start()

    x[t, 0] = out_ref[s]

    def whole(c):
        return pl.ds(c * GROUP, GROUP)

    def part(c, i):
        return pl.ds(c * GROUP + i * half, half)

    def enter(c):
        @pl.when(c == 0)
        def _():
            first = x.at[t, pl.ds(1, GROUP - 1)]
            send(first, first, a2a_send, a2a_recv.at[0], s, right).wait_recv()

        @pl.when(c > 0)
        def _():
            rows = x.at[t, whole(c)]
            send(rows, rows, a2a_send, a2a_recv.at[c], s, right).wait_recv()

        rows = x.at[t, whole(c)]
        for i in range(2):
            to_side(i, rows, rows, ag_send.at[i], ag_recv.at[i, c]).start()

    def relay(c):
        for i in range(2):
            origin = sides[1 - i]
            rows = x.at[origin, whole(c)]
            to_side(i, rows, rows, ag_send.at[i], ag_recv.at[i, c]).wait_recv()
            rows = x.at[origin, part(c, i)]
            to_side(i, rows, rows, relay_send.at[i], relay_recv.at[i, c]).start()

    def compute(c):
        for i in range(2):
            rows = x.at[far, part(c, i)]
            to_side(i, rows, rows, relay_send.at[i], relay_recv.at[i, c]).wait_recv()
        rows = x[:, whole(c)].reshape(tps * GROUP * slots, width)
        gate = jnp.dot(rows, wg[...], preferred_element_type=F32)
        up = jnp.dot(rows, wu[...], preferred_element_type=F32)
        hidden = (gate / (1.0 + jnp.exp(-gate)) * up).astype(BF16)
        made = jnp.dot(hidden, wd[...], preferred_element_type=F32)
        p[:, whole(c)] = made.astype(BF16).reshape(tps, GROUP, slots, width)
        for i in range(2):
            to_side(
                i, p.at[far, part(c, i)], r_in.at[i, pl.ds(c * half, half)],
                r_send.at[i], r_recv.at[i, c],
            ).start()

    def pass_on(c):
        for i in range(2):
            got = r_in.at[i, pl.ds(c * half, half)]
            to_side(i, got, got, r_send.at[i], r_recv.at[i, c]).wait_recv()
            mine = p[sides[i], part(c, i)].astype(F32)
            p[sides[i], part(c, i)] = (mine + got[...].astype(F32)).astype(BF16)
        for i in range(2):
            to_side(
                i, p.at[sides[i], whole(c)], m_in.at[i, whole(c)], m_send.at[i], m_recv.at[i, c]
            ).start()

    def leave(c):
        total = p[t, whole(c)].astype(F32)
        for i in range(2):
            got = m_in.at[i, whole(c)]
            to_side(i, got, got, m_send.at[i], m_recv.at[i, c]).wait_recv()
            total = total + got[...].astype(F32)
        p[t, whole(c)] = total.astype(BF16)

        @pl.when(c == 0)
        def _():
            ret_ref[s] = p[t, 0]

        @pl.loop(jnp.where(c == 0, 1, 0), GROUP)
        def _(j):
            k = c * GROUP + j
            to = lax.rem(s + experts - k, experts)
            send(p.at[t, k], ret_ref.at[s], ret_send, ret_recv, to, t).start()

    @pl.loop(0, steps + 4)
    def _(i):
        @pl.when(i < steps)
        def _():
            enter(i)

        @pl.when((i >= 1) & (i < steps + 1))
        def _():
            relay(i - 1)

        @pl.when(i >= 4)
        def _():
            leave(i - 4)

        @pl.when((i >= 3) & (i < steps + 3))
        def _():
            pass_on(i - 3)

        @pl.when(i == 2)
        def _():
            for load in loads[2:]:
                load.wait()

        @pl.when((i >= 2) & (i < steps + 2))
        def _():
            compute(i - 2)

    most = x.at[0, pl.ds(0, experts - 1)]
    every = x.at[0]
    some = x.at[0, pl.ds(0, experts // 2)]
    back = ret_ref.at[pl.ds(0, experts - 1)]
    send(most, back, a2a_send, ret_recv, s, right).wait_send()
    send(most, back, ret_send, ret_recv, s, right).wait()
    for i in range(2):
        to_side(i, every, every, ag_send.at[i], ag_recv.at[i, 0]).wait_send()
        to_side(i, some, some, relay_send.at[i], relay_recv.at[i, 0]).wait_send()
        to_side(i, some, some, r_send.at[i], r_recv.at[i, 0]).wait_send()
        to_side(i, every, every, m_send.at[i], m_recv.at[i, 0]).wait_send()
    spread = spread_ref[...]
    results = ret_ref[...].reshape(experts * slots, width)
    mixed = stream[...].astype(F32)
    for _ in range(3):
        digit = spread.astype(BF16)
        mixed = mixed + jnp.dot(digit, results, preferred_element_type=F32)
        spread = spread - digit.astype(F32)
    mixed_ref[...] = mixed.astype(BF16)


def at_experts(normed, out_weight, resid, norm_gain, routes, route_weights, w_gate, w_up, w_down):
    groups, tps = normed.shape[:2]
    rows, width = resid.shape
    hidden = w_gate.shape[2]
    experts = lax.axis_size("sp")
    slots = 16
    steps = experts // GROUP
    vmem = pl.BlockSpec(memory_space=pltpu.VMEM)
    hbm = pl.BlockSpec(memory_space=pltpu.HBM)
    dma = pltpu.SemaphoreType.DMA
    return pl.pallas_call(
        experts_kernel,
        out_shape=jax.ShapeDtypeStruct((rows, width), BF16),
        in_specs=[vmem, hbm, hbm, vmem, vmem, vmem, hbm, hbm, hbm],
        out_specs=vmem,
        scratch_shapes=[
            pltpu.VMEM((groups * tps, 64, 128), BF16),
            pltpu.VMEM(out_weight.shape, BF16),
            pltpu.VMEM((rows, width), BF16),
            pltpu.VMEM((rows, width), BF16),
            pltpu.VMEM((rows, experts * slots), F32),
            pltpu.VMEM((experts, slots, width), BF16),
            pltpu.VMEM((experts, slots, width), BF16),
            pltpu.VMEM((tps, experts, slots, width), BF16),
            pltpu.VMEM((tps, experts, slots, width), BF16),
            pltpu.VMEM((2, experts // 2, slots, width), BF16),
            pltpu.VMEM((2, experts, slots, width), BF16),
            pltpu.VMEM((width, hidden), BF16),
            pltpu.VMEM((width, hidden), BF16),
            pltpu.VMEM((hidden, width), BF16),
            dma((5,)),
            dma,
            dma,
            dma,
            dma((steps,)),
            dma((2,)),
            dma((2, steps)),
            dma((2,)),
            dma((2, steps)),
            dma((2,)),
            dma((2, steps)),
            dma((2,)),
            dma((2, steps)),
            dma,
            dma,
        ],
        compiler_params=pltpu.CompilerParams(
            collective_id=1, has_side_effects=True, vmem_limit_bytes=52 * 1024 * 1024
        ),
        name="experts",
    )(
        normed, out_weight, resid, norm_gain.reshape(1, width), routes.T, route_weights.T,
        w_gate, w_up, w_down,
    )


def on_device(
    queries,
    keys,
    values,
    cum_gate,
    documents,
    head_gain,
    out_weight,
    resid,
    norm_gain,
    routes,
    route_weights,
    w_gate,
    w_up,
    w_down,
):
    tokens = queries.shape[0]
    heads = cum_gate.shape[1]
    sp_count = lax.axis_size("sp")
    members = sp_count // heads
    qkv = jnp.concatenate([queries, keys, values], axis=0)
    gain_row = jnp.pad(head_gain, (0, tokens - head_gain.shape[0]))
    small = jnp.concatenate(
        [cum_gate.T, documents.astype(F32)[None], gain_row[None]], axis=0
    )
    q, kvx = gather_history(qkv, small, heads, members)
    normed = attend(q, kvx, small)
    return at_experts(
        normed, out_weight, resid, norm_gain, routes, route_weights, w_gate, w_up, w_down
    )


def solution(mesh):
    in_specs = (
        P("sp", "tp"),
        P("sp", "tp"),
        P("sp", "tp"),
        P("sp", "tp"),
        P("sp"),
        P("tp"),
        P(),
        P(("sp", "tp"), None),
        P(),
        P(("sp", "tp"), None),
        P(("sp", "tp"), None),
        P("sp", None, "tp"),
        P("sp", None, "tp"),
        P("sp", "tp", None),
    )
    out_specs = P(("sp", "tp"), None)
    return jax.shard_map(
        on_device, mesh=mesh, in_specs=in_specs, out_specs=out_specs, check_vma=False
    )
```
